32 devices in a mesh: sp: 8 (over z, y), tp: 4 (over x, core).
Axes of the slice: x: 2, y: 2, z: 4, core: 2. Of those that a mesh axis runs over, the one named last changes fastest.
Arguments:
- queries: bfloat16 [4096, 1024], P('sp', 'tp'), may hold values from -6 to 6
- keys: bfloat16 [4096, 1024], P('sp', 'tp'), may hold values from -6 to 6
- values: bfloat16 [4096, 1024], P('sp', 'tp'), may hold values from -6 to 6
- output_gate_logits: bfloat16 [4096, 1024], P('sp', 'tp'), may hold values from -6 to 6
- input_gate_log: float32 [4096, 8], P('sp', 'tp'), may hold values from -5 to 125
- forget_gate_logits: float32 [4096, 8], P('sp', 'tp')
- extra_decay_log: float32 [4096, 8], P('sp', 'tp'), may hold values from -1 to 0
- document: int32 [4096], P('sp'), may hold values from 0 to 3, never falling along the last dimension, each value on 1 to 2048 neighbouring positions
- residual: bfloat16 [4096, 2048], P('sp', 'tp'), may hold values from -16 to 16
- cell_norm_gain: bfloat16 [1024], P('tp'), may hold values from 0.099609375 to 1.8984375
- output_weight: bfloat16 [1024, 2048], P('tp'), may hold values from -0.1875 to 0.1875
- mixer_norm_gain: bfloat16 [2048], P('tp'), may hold values from 0.099609375 to 1.8984375
- up_weight: bfloat16 [2048, 8192], P('sp', 'tp'), may hold values from -0.125 to 0.125
- down_weight: bfloat16 [8192, 2048], P('tp', 'sp'), may hold values from -0.0625 to 0.0625
Outputs:
- layer_out: bfloat16 [4096, 2048], P('sp', 'tp')
The draws below stay inside these ranges and needn't reach their ends.
All inputs are finite; a program needn't handle non-finite values.
Results may differ from the reference program's by a relative error of at most 0.015.
Values may be sent and summed in bfloat16 or wider, within the bound.
A program may use at most 128 MiB of HBM per device.

```python
import math
import jax
import jax.numpy as jnp
import numpy as np
from jax import lax

D = 2048
FF = 8192
HM = 8
DH = 128
BLOCK = 128
TOK_DEV = 512
TOKENS = 4096
DOCS = 4
MOST = 2048
N_SP = 8
N_TP = 4


def draw_input_gate_log(key, part):
    key_base = jax.random.fold_in(key, 0)
    return jnp.clip(jax.random.normal(key_base, (TOKENS, HM), jnp.float32), -4.0, 4.0)


def draw_forget_gate_logits(key, part):
    key_kind, key_device, key_noise = jax.random.split(key, 3)
    fast_heads = jax.random.randint(key_kind, (HM,), 0, 2) == 1
    device_rate = jax.random.uniform(key_device, (TOKENS // TOK_DEV, 1, 1), jnp.float32, 0.0, math.log(4.0))
    jitter = jax.random.uniform(key_noise, (TOKENS // TOK_DEV, TOK_DEV, HM), jnp.float32, -0.7, 0.7)
    slow_pre = math.log(8.0 * MOST) - device_rate + jitter
    fast_pre = math.log(40.0) + jitter
    result = jnp.where(fast_heads[None, None, :], fast_pre, slow_pre)
    return result.reshape(TOKENS, HM)


def draw_extra_decay_log(key, part):
    key_spot, key_head, key_depth = jax.random.split(key, 3)
    places = max(TOKENS // TOK_DEV * 2, 4)
    spots = jax.random.randint(key_spot, (places,), 0, TOKENS)
    heads_hit = jax.random.randint(key_head, (places,), 0, HM)
    depths = jax.random.uniform(key_depth, (places,), jnp.float32, math.log(0.5), math.log(0.8))
    return jnp.zeros((TOKENS, HM), jnp.float32).at[spots, heads_hit].min(depths)


def draw_residual(key, part):
    key_values = jax.random.fold_in(key, 0)
    ramp = jnp.exp(jnp.linspace(0.0, math.log(3.0), D)).astype(jnp.float32)
    entries = jnp.clip(jax.random.normal(key_values, (TOKENS, D), jnp.float32), -4.0, 4.0)
    return (entries * ramp[None, :] / 1.7).astype(jnp.bfloat16)


def shard_levels(rng, dims, cuts, smallest, high):
    loudness = 1.0
    for axis_at, parts in cuts:
        draws = jax.random.uniform(jax.random.fold_in(jax.random.fold_in(rng, 6), axis_at), (parts,), jnp.float32, smallest / len(cuts), high / len(cuts))
        loudness = loudness * jnp.repeat(jnp.exp(draws), dims[axis_at] // parts).reshape((-1,) + (1,) * (len(dims) - 1 - axis_at))
    return loudness


def split_up(amount, total, most, slope):
    portions = [(1 << 20) // math.isqrt(grade ** slope) + 1 for grade in range(2, amount + 1)]
    surplus, counts = total - most - (amount - 1), [1] * (amount - 1)
    while surplus > 0:
        free = [i for i in range(amount - 1) if counts[i] < most]
        mass, budget = sum([portions[i] for i in free]), surplus
        for i in free:
            more = min(most - counts[i], max(1, budget * portions[i] // mass), surplus)
            counts[i] = counts[i] + more
            surplus = surplus - more
    return np.array([most] + counts)


def ragged_sizes(stream_key, count, total, limit, lean):
    if count == 2:
        one = jax.random.randint(stream_key, (), max(1, total - limit), min(limit, total - 1) + 1)
        return jnp.stack([one, total - one])
    lengths = jnp.asarray(split_up(count, total, limit, lean), jnp.int32)
    couples = (count - 1) // 2
    source_of, receiver = lengths[1:1 + 2 * couples:2], lengths[2:2 + 2 * couples:2]
    slack = jnp.minimum(source_of - 1, limit - receiver)
    passed = jax.random.randint(jax.random.fold_in(stream_key, 1), (couples,), 0, 1 << 20) % (slack + 1)
    lengths = lengths.at[1:1 + 2 * couples:2].set(source_of - passed).at[2:2 + 2 * couples:2].set(receiver + passed)
    return lengths[jax.random.permutation(jax.random.fold_in(stream_key, 2), count)]


def gaussian(key, extent, scale, bound, cuts=(), dtype=jnp.bfloat16):
    values = jax.random.normal(key, extent, jnp.float32) * scale
    if len(cuts) > 0:
        values = shard_levels(key, extent, cuts, -0.22, 0.18) * values
    return jnp.clip(values, min=-bound, max=bound).astype(dtype)


def setup_inputs(seed: int = 0) -> dict:
    streams_of = jax.random.split(jax.random.key(seed), 15)
    queries = gaussian(streams_of[0], (TOKENS, HM * DH), 1.0, 6.0, ((0, 8), (1, 4)))
    keys = gaussian(streams_of[1], (TOKENS, HM * DH), 1.0, 6.0, ((0, 8), (1, 4)))
    values = gaussian(streams_of[2], (TOKENS, HM * DH), 1.0, 6.0, ((0, 8), (1, 4)))
    output_gate_logits = gaussian(streams_of[3], (TOKENS, HM * DH), 1.0, 6.0, ((0, 8), (1, 4)))
    input_gate_log = draw_input_gate_log(jax.random.fold_in(streams_of[14], 71), 0)
    forget_gate_logits = draw_forget_gate_logits(jax.random.fold_in(streams_of[14], 71), 0)
    extra_decay_log = draw_extra_decay_log(jax.random.fold_in(streams_of[14], 71), 0)
    document = jnp.searchsorted(jnp.cumsum(ragged_sizes(streams_of[7], DOCS, TOKENS, MOST, 0)), jnp.arange(TOKENS), side="right").astype(jnp.int32)
    residual = draw_residual(jax.random.fold_in(streams_of[14], 71), 0)
    cell_norm_gain = jnp.clip(1.0 + 0.18 * jax.random.normal(streams_of[9], (HM * DH,), jnp.float32), 0.099609375, 1.8984375).astype(jnp.bfloat16)
    output_weight = gaussian(streams_of[10], (HM * DH, D), (HM * DH) ** -0.5, 0.1875, ((0, 4),))
    mixer_norm_gain = jnp.clip(1.0 + 0.18 * jax.random.normal(streams_of[11], (D,), jnp.float32), 0.099609375, 1.8984375).astype(jnp.bfloat16)
    up_weight = gaussian(streams_of[12], (D, FF), D ** -0.5, 0.125, ((0, 8), (1, 4)))
    down_weight = gaussian(streams_of[13], (FF, D), FF ** -0.5, 0.0625, ((0, 4), (1, 8)))
    return dict(queries=queries, keys=keys, values=values, output_gate_logits=output_gate_logits, input_gate_log=input_gate_log, forget_gate_logits=forget_gate_logits, extra_decay_log=extra_decay_log, document=document, residual=residual, cell_norm_gain=cell_norm_gain, output_weight=output_weight, mixer_norm_gain=mixer_norm_gain, up_weight=up_weight, down_weight=down_weight)


NEG = -1e+30
EPS = 1e-06
HIGH = lax.Precision.HIGHEST

def block_terms(carry, inputs):
    memory, normer, stabil, last_doc = carry
    q_blk, k_blk, v_blk, gate_in, gate_log, doc_blk = inputs
    length = doc_blk.shape[0]
    causal = jnp.arange(length)[:, None] >= jnp.arange(length)[None, :]
    cumulative = jnp.cumsum(gate_log, axis=-1)
    same_doc = (doc_blk[:, None] == doc_blk[None, :]) & causal
    pair_log = cumulative[:, :, None] - cumulative[:, None, :] + gate_in[:, None, :]
    pair_log = jnp.where(same_doc[None], pair_log, NEG)
    live_rows = doc_blk == last_doc
    carried_log = jnp.where(live_rows[None, :], cumulative + stabil[:, None], NEG)
    peak_log = jnp.maximum(carried_log, lax.optimization_barrier(jnp.max(pair_log, axis=-1)))
    weights = jnp.exp(pair_log - peak_log[:, :, None])
    carried = jnp.exp(carried_log - peak_log)
    scores = jnp.einsum('htd,hsd->hts', q_blk, k_blk, precision=HIGH) * weights
    numerator = carried[:, :, None] * jnp.einsum('htd,hde->hte', q_blk, memory, precision=HIGH)
    numerator = numerator + jnp.einsum('hts,hse->hte', scores, v_blk, precision=HIGH)
    denominator = carried * jnp.einsum('htd,hd->ht', q_blk, normer, precision=HIGH) + lax.optimization_barrier(jnp.sum(scores, axis=-1))
    end_doc = doc_blk[-1]
    end_cum = cumulative[:, -1]
    keep_log = jnp.where((doc_blk == end_doc)[None, :], end_cum[:, None] - cumulative + gate_in, NEG)
    old_log = jnp.where(last_doc == end_doc, end_cum + stabil, NEG)
    new_stab = jnp.maximum(old_log, lax.optimization_barrier(jnp.max(keep_log, axis=-1)))
    scaled = jnp.exp(keep_log - new_stab[:, None])
    decayed = jnp.exp(old_log - new_stab)
    memory = decayed[:, None, None] * memory + jnp.einsum('hs,hsd,hse->hde', scaled, k_blk, v_blk, precision=HIGH)
    normer = decayed[:, None] * normer + jnp.einsum('hs,hsd->hd', scaled, k_blk, precision=HIGH)
    return ((memory, normer, new_stab, end_doc), (numerator, denominator, peak_log, cumulative))

def split_heads(source, blocks):
    return source.astype(jnp.float32).reshape(blocks, BLOCK, -1, DH).transpose(0, 2, 1, 3)

def split_gates(source, blocks):
    return source.reshape(blocks, BLOCK, -1).transpose(0, 2, 1)

def within_block_pass(queries, keys, values, input_gate_log, forget_gate_logits, extra_decay_log, document):
    blocks = queries.shape[0] // BLOCK
    head_count = queries.shape[1] // DH
    query_heads = split_heads(queries, blocks) * DH ** (-0.5)
    forget_log_values = jax.nn.log_sigmoid(forget_gate_logits) + extra_decay_log
    inputs = (query_heads, split_heads(keys, blocks), split_heads(values, blocks), split_gates(input_gate_log, blocks), split_gates(forget_log_values, blocks), document.reshape(blocks, BLOCK))
    initial = (jnp.zeros((head_count, DH, DH), jnp.float32), jnp.zeros((head_count, DH), jnp.float32), jnp.full((head_count,), NEG, jnp.float32), jnp.array(-1, jnp.int32))
    final_state, output_rows = lax.scan(block_terms, initial, inputs)
    return (query_heads, final_state, output_rows)

def head_mix(cell_out, output_gate_logits, cell_norm_gain):
    row_count = output_gate_logits.shape[0]
    head_count = cell_out.shape[1]
    hidden = cell_out.transpose(0, 2, 1, 3).reshape(row_count, head_count * DH)
    inverse = lax.rsqrt(lax.optimization_barrier(jnp.mean(hidden * hidden, axis=1, keepdims=True)) + EPS)
    gated = jax.nn.sigmoid(output_gate_logits.astype(jnp.float32))
    gains = cell_norm_gain.astype(jnp.float32)
    return (gated * hidden * inverse * gains[None, :]).astype(jnp.bfloat16)

def reference(queries, keys, values, output_gate_logits, input_gate_log, forget_gate_logits, extra_decay_log, document, residual, cell_norm_gain, output_weight, mixer_norm_gain, up_weight, down_weight):
    query_heads, final_state, output_rows = within_block_pass(queries, keys, values, input_gate_log, forget_gate_logits, extra_decay_log, document)
    numerator, denominator, peak_log, cumulative = output_rows
    cell_out = numerator / jnp.maximum(jnp.abs(denominator), 1.0)[..., None]
    mixed = head_mix(cell_out, output_gate_logits, cell_norm_gain)
    out_groups = output_weight.reshape(N_TP, -1, D).astype(jnp.float32)
    down_groups = down_weight.reshape(N_TP, -1, D).astype(jnp.float32)
    gain_wide = mixer_norm_gain.astype(jnp.float32)

    def rows_step(row_args):
        mixed_rows, resid_rows = row_args
        row_count = mixed_rows.shape[0]
        group_parts = jnp.einsum('rgk,gkd->grd', mixed_rows.reshape(row_count, N_TP, -1).astype(jnp.float32), out_groups)
        group_parts = lax.optimization_barrier(group_parts.astype(jnp.bfloat16)).astype(jnp.float32)
        first_sum = (resid_rows.astype(jnp.float32) + lax.optimization_barrier(jnp.sum(group_parts, axis=0))).astype(jnp.bfloat16)
        first_wide = lax.optimization_barrier(first_sum).astype(jnp.float32)
        inverse = lax.rsqrt(lax.optimization_barrier(jnp.mean(first_wide * first_wide, axis=1, keepdims=True)) + EPS)
        normed = (first_wide * inverse * gain_wide).astype(jnp.bfloat16)
        hidden = jnp.dot(normed, up_weight, preferred_element_type=jnp.float32)
        squared = jnp.square(jax.nn.relu(hidden)).astype(jnp.bfloat16)
        channel_parts = jnp.einsum('rgf,gfd->grd', squared.reshape(row_count, N_TP, -1).astype(jnp.float32), down_groups)
        channel_parts = lax.optimization_barrier(channel_parts.astype(jnp.bfloat16)).astype(jnp.float32)
        return (first_wide + lax.optimization_barrier(jnp.sum(channel_parts, axis=0))).astype(jnp.bfloat16)
    layer = lax.map(rows_step, (mixed.reshape(N_SP, -1, mixed.shape[1]), residual.reshape(N_SP, -1, D)))
    return layer.reshape(-1, D)
```

```python
import functools

import jax
import jax.numpy as jnp
from jax import lax
from jax.experimental import pallas as pl
from jax.experimental.pallas import tpu as pltpu
from jax.sharding import PartitionSpec as P

DH = 128
BLOCK = 128
MOST = 2048


NEG = -1e30
EPS = 1e-06
HIGH = lax.Precision.HIGHEST


def carried_in(value, axis, join, neutral):
    count, mine = (lax.axis_size(axis), lax.axis_index(axis))
    pieces = jax.tree.map(lambda part: lax.all_gather(part, axis), value)
    subtotal = jax.tree.map(
        lambda part, zero: jnp.full_like(part, 0) + jnp.asarray(zero, part.dtype), value, neutral
    )

    def step(position, subtotal):
        longer = join(subtotal, jax.tree.map(lambda part: part[position], pieces))
        return jax.tree.map(lambda new, old: jnp.where(position < mine, new, old), longer, subtotal)

    return lax.fori_loop(0, count - 1, step, subtotal)


def block_terms(carry, inputs):
    memory, normer, stabil, last_doc = carry
    q_blk, k_blk, v_blk, gate_in, gate_log, doc_blk = inputs
    length = doc_blk.shape[0]
    causal = jnp.arange(length)[:, None] >= jnp.arange(length)[None, :]
    cumulative = jnp.cumsum(gate_log, axis=-1)
    same_doc = (doc_blk[:, None] == doc_blk[None, :]) & causal
    pair_log = cumulative[:, :, None] - cumulative[:, None, :] + gate_in[:, None, :]
    pair_log = jnp.where(same_doc[None], pair_log, NEG)
    live_rows = doc_blk == last_doc
    carried_log = jnp.where(live_rows[None, :], cumulative + stabil[:, None], NEG)
    peak_log = jnp.maximum(carried_log, jnp.max(pair_log, axis=-1))
    weights = jnp.exp(pair_log - peak_log[:, :, None])
    carried = jnp.exp(carried_log - peak_log)
    scores = jnp.einsum("htd,hsd->hts", q_blk, k_blk, precision=HIGH) * weights
    numerator = carried[:, :, None] * jnp.einsum("htd,hde->hte", q_blk, memory, precision=HIGH)
    numerator = numerator + jnp.einsum("hts,hse->hte", scores, v_blk, precision=HIGH)
    denominator = carried * jnp.einsum("htd,hd->ht", q_blk, normer, precision=HIGH) + jnp.sum(
        scores, axis=-1
    )
    end_doc = doc_blk[-1]
    end_cum = cumulative[:, -1]
    keep_log = jnp.where(
        (doc_blk == end_doc)[None, :], end_cum[:, None] - cumulative + gate_in, NEG
    )
    old_log = jnp.where(last_doc == end_doc, end_cum + stabil, NEG)
    new_stab = jnp.maximum(old_log, jnp.max(keep_log, axis=-1))
    scaled = jnp.exp(keep_log - new_stab[:, None])
    decayed = jnp.exp(old_log - new_stab)
    memory = decayed[:, None, None] * memory + jnp.einsum(
        "hs,hsd,hse->hde", scaled, k_blk, v_blk, precision=HIGH
    )
    normer = decayed[:, None] * normer + jnp.einsum("hs,hsd->hd", scaled, k_blk, precision=HIGH)
    return ((memory, normer, new_stab, end_doc), (numerator, denominator, peak_log, cumulative))


def split_heads(source, blocks):
    return source.astype(jnp.float32).reshape(blocks, BLOCK, -1, DH).transpose(0, 2, 1, 3)


def split_gates(source, blocks):
    return source.reshape(blocks, BLOCK, -1).transpose(0, 2, 1)


def within_block_pass(
    queries, keys, values, input_gate_log, forget_gate_logits, extra_decay_log, document
):
    blocks = queries.shape[0] // BLOCK
    head_count = queries.shape[1] // DH
    query_heads = split_heads(queries, blocks) * DH ** (-0.5)
    forget_log_values = jax.nn.log_sigmoid(forget_gate_logits) + extra_decay_log
    inputs = (
        query_heads,
        split_heads(keys, blocks),
        split_heads(values, blocks),
        split_gates(input_gate_log, blocks),
        split_gates(forget_log_values, blocks),
        document.reshape(blocks, BLOCK),
    )
    initial = (
        jnp.zeros((head_count, DH, DH), jnp.float32),
        jnp.zeros((head_count, DH), jnp.float32),
        jnp.full((head_count,), NEG, jnp.float32),
        jnp.array(-1, jnp.int32),
    )
    final_state, output_rows = lax.scan(block_terms, initial, inputs)
    return (query_heads, final_state, output_rows)


def head_mix(cell_out, output_gate_logits, cell_norm_gain):
    row_count = output_gate_logits.shape[0]
    head_count = cell_out.shape[1]
    hidden = cell_out.transpose(0, 2, 1, 3).reshape(row_count, head_count * DH)
    squares = lax.psum(jnp.sum(hidden * hidden, axis=1), "tp")
    inverse = lax.rsqrt(squares / (head_count * DH * lax.axis_size("tp")) + EPS)
    gated = jax.nn.sigmoid(output_gate_logits.astype(jnp.float32))
    gains = cell_norm_gain.astype(jnp.float32)
    return (gated * hidden * inverse[:, None] * gains[None, :]).astype(jnp.bfloat16)


def join_states(earlier, later):
    mem_a, norm_a, stab_a, log_a, first_a, last_a = earlier
    mem_b, norm_b, stab_b, log_b, first_b, last_b = later
    joined = last_a == last_b
    stab_ab = jnp.where(joined, jnp.maximum(log_b + stab_a, stab_b), stab_b)
    weight_a = jnp.where(joined, jnp.exp(log_b + stab_a - stab_ab), 0.0)
    weight_b = jnp.exp(stab_b - stab_ab)
    memory = weight_a[:, None, None] * mem_a + weight_b[:, None, None] * mem_b
    normer = weight_a[:, None] * norm_a + weight_b[:, None] * norm_b
    blank_b = last_b < 0
    memory = jnp.where(blank_b, mem_a, memory)
    normer = jnp.where(blank_b, norm_a, normer)
    stabil = jnp.where(blank_b, stab_a, stab_ab)
    first_doc = jnp.where(first_a < 0, first_b, first_a)
    last_doc = jnp.where(blank_b, last_a, last_b)
    return (memory, normer, stabil, log_a + log_b, first_doc, last_doc)


def local(
    queries,
    keys,
    values,
    output_gate_logits,
    input_gate_log,
    forget_gate_logits,
    extra_decay_log,
    document,
    residual,
    cell_norm_gain,
    output_weight,
    mixer_norm_gain,
    up_weight,
    down_weight,
):
    query_heads, final_state, output_rows = within_block_pass(
        queries, keys, values, input_gate_log, forget_gate_logits, extra_decay_log, document
    )
    numerator, denominator, peak_log, cumulative = output_rows
    memory, normer, stabil, last_doc = final_state
    step_logs = cumulative[:, :, -1]
    offsets = jnp.cumsum(step_logs, axis=0) - step_logs
    through = cumulative + offsets[:, :, None]
    summary = (memory, normer, stabil, jnp.sum(step_logs, axis=0), document[0], last_doc)
    identity = (
        jnp.zeros_like(memory),
        jnp.zeros_like(normer),
        jnp.full_like(stabil, NEG),
        jnp.zeros_like(stabil),
        jnp.array(-1, jnp.int32),
        jnp.array(-1, jnp.int32),
    )
    prefix = carried_in(summary, "sp", join_states, identity)
    doc_blocks = document.reshape(-1, BLOCK)
    carried_log = jnp.where(
        (doc_blocks == prefix[5])[:, None, :], through + prefix[2][None, :, None], NEG
    )
    merged_peak = jnp.maximum(peak_log, carried_log)
    own_weight = jnp.exp(peak_log - merged_peak)
    far_weight = jnp.exp(carried_log - merged_peak)
    numerator = own_weight[..., None] * numerator + far_weight[..., None] * jnp.einsum(
        "nhtd,hde->nhte", query_heads, prefix[0], precision=HIGH
    )
    denominator = own_weight * denominator + far_weight * jnp.einsum(
        "nhtd,hd->nht", query_heads, prefix[1], precision=HIGH
    )
    cell_out = numerator / jnp.maximum(jnp.abs(denominator), 1.0)[..., None]
    mixed = head_mix(cell_out, output_gate_logits, cell_norm_gain)
    head_terms = jnp.dot(mixed, output_weight, preferred_element_type=jnp.float32)
    width = residual.shape[1]
    model_width = width * lax.axis_size("tp")
    own_sum = lax.psum_scatter(
        head_terms.astype(jnp.bfloat16), "tp", scatter_dimension=1, tiled=True
    ).astype(jnp.float32)
    first_sum = (residual.astype(jnp.float32) + own_sum).astype(jnp.bfloat16)
    first_wide = lax.optimization_barrier(first_sum).astype(jnp.float32)
    squares = lax.psum(jnp.sum(first_wide * first_wide, axis=1), "tp")
    inverse = lax.rsqrt(squares / model_width + EPS)
    normed_own = (first_wide * inverse[:, None] * mixer_norm_gain.astype(jnp.float32)).astype(
        jnp.bfloat16
    )
    normed_full = lax.all_gather(normed_own, "tp", axis=1, tiled=True)
    hidden = jnp.dot(
        normed_full,
        lax.all_gather(up_weight, "sp", axis=0, tiled=True),
        preferred_element_type=jnp.float32,
    )
    squared = jnp.square(jax.nn.relu(hidden)).astype(jnp.bfloat16)
    channel = jnp.dot(
        squared,
        lax.all_gather(down_weight, "sp", axis=1, tiled=True),
        preferred_element_type=jnp.float32,
    )
    own_channel = lax.psum_scatter(
        channel.astype(jnp.bfloat16), "tp", scatter_dimension=1, tiled=True
    ).astype(jnp.float32)
    return (lax.optimization_barrier(first_sum).astype(jnp.float32) + own_channel).astype(
        jnp.bfloat16
    )


MESH = pl.DeviceIdType.MESH
F32 = jnp.float32
BF16 = jnp.bfloat16
STATE_ROWS = DH + 8


def to_columns(rows):
    pad = jnp.zeros((128 - rows.shape[0], rows.shape[1]), F32)
    return jnp.transpose(jnp.concatenate([rows, pad], axis=0))


def row_sums(wide):
    ones = jnp.ones((8, wide.shape[1]), F32)
    return lax.dot_general(
        ones, wide, (((1,), (1,)), ((), ())), precision=HIGH, preferred_element_type=F32
    )


def layer_kernel(
    n,
    m,
    back,
    q_ref,
    k_ref,
    v_ref,
    og_ref,
    gates_ref,
    resid_ref,
    cgain_ref,
    wout_ref,
    mgain_ref,
    up_ref,
    down_ref,
    out_ref,
    up_all,
    down_all,
    state_out,
    state_in,
    y_ref,
    terms_out,
    terms_in,
    squares_out,
    squares_in,
    first_ref,
    normed,
    sums_out,
    sums_in,
    squared,
    parts_out,
    parts_in,
    ring_send,
    ring_recv,
    state_send,
    state_recv,
    terms_send,
    terms_recv,
    squares_send,
    squares_recv,
    normed_send,
    normed_recv,
    sums_send,
    sums_recv,
    parts_send,
    parts_recv,
):
    sp, tp = lax.axis_index("sp"), lax.axis_index("tp")
    rows, heads = q_ref.shape[0], q_ref.shape[1] // DH
    depth, hidden_width = up_ref.shape
    half, quarter = depth // 2, depth // 4
    width = resid_ref.shape[1]
    per_owner = width // depth

    def index_of(position):
        late = position // (n // 2)
        return (1 - late) * 2 * position + late * (2 * (n - 1 - position) + 1)

    odd = sp % 2
    place = (1 - odd) * (sp // 2) + odd * (n - 1 - sp // 2)
    target = (index_of((place + 1) % n), index_of((place + n - 1) % n))

    barrier = pltpu.get_barrier_semaphore()
    for k in range(1, n):
        pl.semaphore_signal(barrier, device_id=((sp + k) % n, tp), device_id_type=MESH)
    for k in range(1, m):
        pl.semaphore_signal(barrier, device_id=(sp, (tp + k) % m), device_id_type=MESH)
    pl.semaphore_wait(barrier, n + m - 2)

    def block_at(way, step):
        return index_of((place + (n - step if way == 0 else step)) % n)

    def ring(stream, way, step, sub):
        block = block_at(way, step)
        if stream == 0:
            inner = way * half + sub * quarter
            where = pl.ds(pl.multiple_of(block * depth + inner, quarter), quarter)
            dst = up_all.at[where, :]
            src = up_ref.at[pl.ds(inner, quarter), :] if step == 0 else dst
        else:
            deep = pl.ds(sub * (hidden_width // 2), hidden_width // 2)
            dst = down_all.at[block, way, deep, :]
            src = down_ref.at[deep, pl.ds(way * half, half)] if step == 0 else dst
        return pltpu.make_async_remote_copy(
            src_ref=src,
            dst_ref=dst,
            send_sem=ring_send.at[stream, way, step, sub],
            recv_sem=ring_recv.at[stream, way, step, sub],
            device_id=(target[way], tp),
            device_id_type=MESH,
        )

    def arrived(stream, way, step, sub):
        block = block_at(way, step + 1)
        if stream == 0:
            inner = way * half + sub * quarter
            dst = up_all.at[pl.ds(pl.multiple_of(block * depth + inner, quarter), quarter), :]
        else:
            dst = down_all.at[block, way, pl.ds(sub * (hidden_width // 2), hidden_width // 2), :]
        pltpu.make_async_remote_copy(
            src_ref=dst,
            dst_ref=dst,
            send_sem=ring_send.at[stream, way, step, sub],
            recv_sem=ring_recv.at[stream, way, step, sub],
            device_id=(target[way], tp),
            device_id_type=MESH,
        ).wait_recv()

    def open_stream(stream):
        for sub in range(2):
            for way in range(2):
                ring(stream, way, 0, sub).start()

    events = [(a, b, c) for a in range(2) for b in range(n - 1) for c in range(2)]
    done = [0]

    def pump():
        stream, step, sub = events[done[0]]
        done[0] += 1
        for way in range(2):
            arrived(stream, way, step, sub)
            if step + 1 < n - 1:
                ring(stream, way, step + 1, sub).start()
        if stream == 0 and step == n - 3 and sub == 1:
            open_stream(1)

    open_stream(0)

    gates = gates_ref[...]
    document = gates[2 * heads : 2 * heads + 1, :]
    across = lax.broadcasted_iota(jnp.int32, (rows, rows), 1)
    along = lax.broadcasted_iota(jnp.int32, (rows, rows), 0)
    upper = (along <= across).astype(F32)
    sums = jnp.dot(gates, upper, precision=HIGH, preferred_element_type=F32)
    last_doc = document[:, rows - 1 : rows]
    totals, stabs, scaled = [], [], []
    for h in range(heads):
        total = sums[h : h + 1, rows - 1 : rows]
        keep = total - sums[h : h + 1, :] + gates[heads + h : heads + h + 1, :]
        keep = jnp.where(document == last_doc, keep, NEG)
        stab = jnp.max(keep, axis=1, keepdims=True)
        totals.append(total)
        stabs.append(stab)
        scaled.append(jnp.exp(keep - stab))
    slab = lax.broadcasted_iota(jnp.int32, (8, rows), 0)
    packed = jnp.broadcast_to(document, (8, rows))
    for h in range(heads):
        packed = jnp.where(slab == h, sums[h : h + 1, :], packed)
        packed = jnp.where(slab == heads + h, scaled[h], packed)
    columns = to_columns(packed)
    doc_col = columns[:, 2 * heads : 2 * heads + 1]
    line = lax.broadcasted_iota(jnp.int32, (8, DH), 0)
    for h in range(heads):
        mine = slice(h * DH, (h + 1) * DH)
        weighted = k_ref[:, mine].astype(F32) * columns[:, heads + h : heads + h + 1]
        state_out[h, 0:DH, :] = jnp.dot(
            jnp.transpose(weighted),
            v_ref[:, mine].astype(F32),
            precision=HIGH,
            preferred_element_type=F32,
        )
        tail = jnp.broadcast_to(jnp.sum(weighted, axis=0, keepdims=True), (8, DH))
        tail = jnp.where(line == 1, stabs[h], tail)
        tail = jnp.where(line == 2, totals[h], tail)
        tail = jnp.where(line == 3, last_doc, tail)
        state_out[h, DH : DH + 8, :] = tail

    def state_copy(k):
        return pltpu.make_async_remote_copy(
            src_ref=state_out,
            dst_ref=state_in.at[k - 1],
            send_sem=state_send.at[k - 1],
            recv_sem=state_recv.at[k - 1],
            device_id=((sp + k) % n, tp),
            device_id_type=MESH,
        )

    for k in range(1, back + 1):
        state_copy(k).start()

    own_rows = pl.ds(pl.multiple_of(sp * depth, depth), depth)
    up_all[own_rows, :] = up_ref[...]
    down_all[sp, 0] = down_ref[:, 0:half]
    down_all[sp, 1] = down_ref[:, half:depth]
    pump()

    locals_of = []
    for h in range(heads):
        mine = slice(h * DH, (h + 1) * DH)
        scores = lax.dot_general(
            q_ref[:, mine],
            k_ref[:, mine],
            (((1,), (1,)), ((), ())),
            preferred_element_type=F32,
        ) * (DH**-0.5)
        pair = columns[:, h : h + 1] - sums[h : h + 1, :] + gates[heads + h : heads + h + 1, :]
        pair = jnp.where((doc_col == document) & (along >= across), pair, NEG)
        peak = jnp.max(pair, axis=1, keepdims=True)
        scores = scores * jnp.exp(pair - peak)
        numer = jnp.dot(
            scores, v_ref[:, mine].astype(F32), precision=HIGH, preferred_element_type=F32
        )
        locals_of.append((peak, jnp.sum(scores, axis=1, keepdims=True), numer))
        pump()

    for k in range(1, back + 1):
        state_copy(k).wait_recv()
    first_doc = document[:, 0:1]
    cells = []
    for h in range(heads):
        mine = slice(h * DH, (h + 1) * DH)
        between = jnp.zeros((1, DH), F32)
        logs, valids = [], []
        best = jnp.full((1, DH), NEG, F32)
        for k in range(1, back + 1):
            tail = state_in[k - 1, h, DH : DH + 8, :]
            far = lax.broadcasted_iota(jnp.int32, (1, DH), 1) * 0 + sp
            valid = (tail[3:4, :] == first_doc) & (far >= k)
            log = jnp.where(valid, between + tail[1:2, :], NEG)
            between = between + tail[2:3, :]
            best = jnp.maximum(best, log)
            logs.append(log)
            valids.append(valid)
        memory = jnp.zeros((DH, DH), F32)
        normer = jnp.zeros((1, DH), F32)
        for k in range(1, back + 1):
            weight = jnp.where(valids[k - 1], jnp.exp(logs[k - 1] - best), 0.0)
            memory = memory + jnp.where(
                valids[k - 1], weight * state_in[k - 1, h, 0:DH, :], 0.0
            )
            normer = normer + jnp.where(
                valids[k - 1], weight * state_in[k - 1, h, DH : DH + 1, :], 0.0
            )
        peak, denom, numer = locals_of[h]
        carried = jnp.where(doc_col == first_doc, columns[:, h : h + 1] + best[:, 0:1], NEG)
        merged = jnp.maximum(peak, carried)
        own, other = jnp.exp(peak - merged), jnp.exp(carried - merged)
        query = q_ref[:, mine].astype(F32) * (DH**-0.5)
        numer = own * numer + other * jnp.dot(
            query, memory, precision=HIGH, preferred_element_type=F32
        )
        denom = own * denom + other * jnp.sum(query * normer, axis=1, keepdims=True)
        cell = numer / jnp.maximum(jnp.abs(denom), 1.0)
        cells.append(cell)
        gated = jax.nn.sigmoid(og_ref[:, mine].astype(F32))
        y_ref[:, mine] = (gated * cell * cgain_ref[:, mine].astype(F32)).astype(BF16)
    total = cells[0] * cells[0]
    for h in range(1, heads):
        total = total + cells[h] * cells[h]
    squares_out[...] = row_sums(total)

    def to_peer(src, dst, send_sem, recv_sem, k):
        return pltpu.make_async_remote_copy(
            src_ref=src,
            dst_ref=dst,
            send_sem=send_sem.at[k - 1],
            recv_sem=recv_sem.at[k - 1],
            device_id=(sp, (tp + k) % m),
            device_id_type=MESH,
        )

    def squares_copy(k):
        return to_peer(squares_out, squares_in.at[k - 1], squares_send, squares_recv, k)

    def terms_copy(k):
        return to_peer(terms_out.at[k], terms_in.at[k - 1], terms_send, terms_recv, k)

    def head_term(k):
        owner = (tp + k) % m
        cols = pl.ds(pl.multiple_of(owner * width, width), width)
        return jnp.dot(y_ref[...], wout_ref[:, cols], preferred_element_type=F32).astype(BF16)

    for k in range(1, m):
        squares_copy(k).start()
        terms_out[k] = head_term(k)
        terms_copy(k).start()
    own_term = head_term(0).astype(F32)
    terms_out[0] = own_term.astype(BF16)
    for _ in range(PUMPS_TERMS):
        pump()
    for k in range(1, m):
        squares_copy(k).wait_recv()
        terms_copy(k).wait_recv()
    squares = squares_out[...]
    attn = terms_out[0].astype(F32)
    for k in range(1, m):
        squares = squares + squares_in[k - 1]
        attn = attn + terms_in[k - 1].astype(F32)
    inverse = lax.rsqrt(to_columns(squares)[:, 0:1] / (heads * DH * m) + EPS)
    first = (resid_ref[...].astype(F32) + attn * inverse).astype(BF16)
    first_ref[...] = first
    first = first.astype(F32)
    here = pl.ds(pl.multiple_of(tp * width, width), width)
    normed[:, here] = (first * mgain_ref[...].astype(F32)).astype(BF16)
    sums_out[...] = row_sums(first * first)

    def normed_copy(k):
        return to_peer(normed.at[:, here], normed.at[:, here], normed_send, normed_recv, k)

    def normed_arrival(k):
        source = (tp + m - k) % m
        there = normed.at[:, pl.ds(pl.multiple_of(source * width, width), width)]
        return to_peer(there, there, normed_send, normed_recv, k)

    def sums_copy(k):
        return to_peer(sums_out, sums_in.at[k - 1], sums_send, sums_recv, k)

    for k in range(1, m):
        sums_copy(k).start()
        normed_copy(k).start()
    for _ in range(PUMPS_NORMED):
        pump()
    for k in range(1, m):
        sums_copy(k).wait_recv()
        normed_arrival(k).wait_recv()
    squares = sums_out[...]
    for k in range(1, m):
        squares = squares + sums_in[k - 1]
    scale = lax.rsqrt(to_columns(squares)[:, 0:1] / (width * m) + EPS)
    while done[0] < 2 * (n - 1):
        pump()

    tile = min(hidden_width, 256)
    chunks = hidden_width // tile

    def up_chunk(c, carry):
        cols = pl.ds(pl.multiple_of(c * tile, tile), tile)
        raw = jnp.dot(normed[...], up_all[:, cols], preferred_element_type=F32)
        hidden = jnp.maximum(raw * scale, 0.0)
        squared[:, cols] = (hidden * hidden).astype(BF16)
        return carry

    lax.fori_loop(0, chunks // 2, up_chunk, 0)
    pump()
    lax.fori_loop(chunks // 2, chunks, up_chunk, 0)

    def part_copy(way, step):
        block = block_at(way, step)
        owner, slot = block // per_owner, block % per_owner
        return owner, pltpu.make_async_remote_copy(
            src_ref=parts_out.at[block, way],
            dst_ref=parts_in.at[tp, slot, way],
            send_sem=parts_send.at[block, way],
            recv_sem=parts_recv.at[tp, slot, way],
            device_id=(sp, owner),
            device_id_type=MESH,
        )

    def down_block(step):
        for way in range(2):
            block = block_at(way, step)
            parts_out[block, way] = jnp.dot(
                squared[...], down_all[block, way], preferred_element_type=F32
            ).astype(BF16)
            owner, copy = part_copy(way, step)

            @pl.when(owner != tp)
            def _():
                copy.start()

    down_block(0)
    for step in range(1, n):
        while done[0] < 2 * (n - 1) + 2 * step:
            pump()
        down_block(step)

    for slot in range(per_owner):
        for way in range(2):
            cols = slice(slot * depth + way * half, slot * depth + (way + 1) * half)
            total = parts_out[tp * per_owner + slot, way].astype(F32)
            for k in range(1, m):
                source = (tp + k) % m
                there = parts_in.at[source, slot, way]
                pltpu.make_async_remote_copy(
                    src_ref=there,
                    dst_ref=there,
                    send_sem=parts_send.at[0, 0],
                    recv_sem=parts_recv.at[source, slot, way],
                    device_id=(sp, source),
                    device_id_type=MESH,
                ).wait_recv()
                total = total + parts_in[source, slot, way].astype(F32)
            out_ref[:, cols] = (first_ref[:, cols].astype(F32) + total).astype(BF16)

    for stream, step, sub in events:
        for way in range(2):
            ring(stream, way, step, sub).wait_send()
    for k in range(1, back + 1):
        state_copy(k).wait_send()
    for k in range(1, m):
        squares_copy(k).wait_send()
        terms_copy(k).wait_send()
        sums_copy(k).wait_send()
        normed_copy(k).wait_send()
    for step in range(n):
        for way in range(2):
            owner, copy = part_copy(way, step)

            @pl.when(owner != tp)
            def _():
                copy.wait_send()


PUMPS_TERMS = 4
PUMPS_NORMED = 4


def fused(
    n,
    m,
    queries,
    keys,
    values,
    output_gate_logits,
    input_gate_log,
    forget_gate_logits,
    extra_decay_log,
    document,
    residual,
    cell_norm_gain,
    output_weight,
    mixer_norm_gain,
    up_weight,
    down_weight,
):
    rows, heads = queries.shape[0], queries.shape[1] // DH
    depth, hidden_width = up_weight.shape
    width = residual.shape[1]
    back = min(n - 1, (MOST - 2) // rows + 1)
    forget = jax.nn.log_sigmoid(forget_gate_logits) + extra_decay_log
    gates = jnp.concatenate(
        [forget.T, input_gate_log.T, document.astype(F32)[None, :]], axis=0
    )
    gates = jnp.pad(gates, ((0, 8 - gates.shape[0]), (0, 0)))
    dma = pltpu.SemaphoreType.DMA
    per_owner = width // depth
    return pl.pallas_call(
        functools.partial(layer_kernel, n, m, back),
        out_shape=jax.ShapeDtypeStruct((rows, width), BF16),
        in_specs=[pl.BlockSpec(memory_space=pltpu.VMEM)] * 11,
        out_specs=pl.BlockSpec(memory_space=pltpu.VMEM),
        scratch_shapes=[
            pltpu.VMEM((n * depth, hidden_width), BF16),
            pltpu.VMEM((n, 2, hidden_width, depth // 2), BF16),
            pltpu.VMEM((heads, STATE_ROWS, DH), F32),
            pltpu.VMEM((back, heads, STATE_ROWS, DH), F32),
            pltpu.VMEM((rows, heads * DH), BF16),
            pltpu.VMEM((m, rows, width), BF16),
            pltpu.VMEM((m - 1, rows, width), BF16),
            pltpu.VMEM((8, rows), F32),
            pltpu.VMEM((m - 1, 8, rows), F32),
            pltpu.VMEM((rows, width), BF16),
            pltpu.VMEM((rows, m * width), BF16),
            pltpu.VMEM((8, rows), F32),
            pltpu.VMEM((m - 1, 8, rows), F32),
            pltpu.VMEM((rows, hidden_width), BF16),
            pltpu.VMEM((n, 2, rows, depth // 2), BF16),
            pltpu.VMEM((m, per_owner, 2, rows, depth // 2), BF16),
            dma((2, 2, n - 1, 2)),
            dma((2, 2, n - 1, 2)),
            dma((back,)),
            dma((back,)),
            dma((m - 1,)),
            dma((m - 1,)),
            dma((m - 1,)),
            dma((m - 1,)),
            dma((m - 1,)),
            dma((m - 1,)),
            dma((m - 1,)),
            dma((m - 1,)),
            dma((n, 2)),
            dma((m, per_owner, 2)),
        ],
        compiler_params=pltpu.CompilerParams(
            collective_id=0, has_side_effects=True, vmem_limit_bytes=60 * 1024 * 1024
        ),
        name="layer",
    )(
        queries,
        keys,
        values,
        output_gate_logits,
        gates,
        residual,
        cell_norm_gain[None, :],
        output_weight,
        mixer_norm_gain[None, :],
        up_weight,
        down_weight,
    )


def either(n, m, *args):
    depth, hidden_width = args[12].shape
    heads = args[0].shape[1] // DH
    fits = depth % 256 == 0 and n % 2 == 0 and n >= 4 and n <= 16 and m >= 2
    fits = fits and 2 * heads + 1 <= 8 and args[8].shape[1] % depth == 0
    fits = fits and args[0].shape[0] % 128 == 0 and hidden_width % 256 == 0
    if fits:
        return fused(n, m, *args)
    return local(*args)


def solution(mesh):
    in_specs = (
        P("sp", "tp"),
        P("sp", "tp"),
        P("sp", "tp"),
        P("sp", "tp"),
        P("sp", "tp"),
        P("sp", "tp"),
        P("sp", "tp"),
        P("sp"),
        P("sp", "tp"),
        P("tp"),
        P("tp", None),
        P("tp"),
        P("sp", "tp"),
        P("tp", "sp"),
    )
    out_specs = P("sp", "tp")
    body = functools.partial(either, mesh.shape["sp"], mesh.shape["tp"])
    return jax.shard_map(body, mesh=mesh, in_specs=in_specs, out_specs=out_specs, check_vma=False)
```

```python
import functools

import jax
import jax.numpy as jnp
from jax import lax
from jax.experimental import pallas as pl
from jax.experimental.pallas import tpu as pltpu
from jax.sharding import PartitionSpec as P

DH = 128
BLOCK = 128
MOST = 2048


NEG = -1e30
EPS = 1e-06
HIGH = lax.Precision.HIGHEST


def carried_in(value, axis, join, neutral):
    count, mine = (lax.axis_size(axis), lax.axis_index(axis))
    pieces = jax.tree.map(lambda part: lax.all_gather(part, axis), value)
    subtotal = jax.tree.map(
        lambda part, zero: jnp.full_like(part, 0) + jnp.asarray(zero, part.dtype), value, neutral
    )

    def step(position, subtotal):
        longer = join(subtotal, jax.tree.map(lambda part: part[position], pieces))
        return jax.tree.map(lambda new, old: jnp.where(position < mine, new, old), longer, subtotal)

    return lax.fori_loop(0, count - 1, step, subtotal)


def block_terms(carry, inputs):
    memory, normer, stabil, last_doc = carry
    q_blk, k_blk, v_blk, gate_in, gate_log, doc_blk = inputs
    length = doc_blk.shape[0]
    causal = jnp.arange(length)[:, None] >= jnp.arange(length)[None, :]
    cumulative = jnp.cumsum(gate_log, axis=-1)
    same_doc = (doc_blk[:, None] == doc_blk[None, :]) & causal
    pair_log = cumulative[:, :, None] - cumulative[:, None, :] + gate_in[:, None, :]
    pair_log = jnp.where(same_doc[None], pair_log, NEG)
    live_rows = doc_blk == last_doc
    carried_log = jnp.where(live_rows[None, :], cumulative + stabil[:, None], NEG)
    peak_log = jnp.maximum(carried_log, jnp.max(pair_log, axis=-1))
    weights = jnp.exp(pair_log - peak_log[:, :, None])
    carried = jnp.exp(carried_log - peak_log)
    scores = jnp.einsum("htd,hsd->hts", q_blk, k_blk, precision=HIGH) * weights
    numerator = carried[:, :, None] * jnp.einsum("htd,hde->hte", q_blk, memory, precision=HIGH)
    numerator = numerator + jnp.einsum("hts,hse->hte", scores, v_blk, precision=HIGH)
    denominator = carried * jnp.einsum("htd,hd->ht", q_blk, normer, precision=HIGH) + jnp.sum(
        scores, axis=-1
    )
    end_doc = doc_blk[-1]
    end_cum = cumulative[:, -1]
    keep_log = jnp.where(
        (doc_blk == end_doc)[None, :], end_cum[:, None] - cumulative + gate_in, NEG
    )
    old_log = jnp.where(last_doc == end_doc, end_cum + stabil, NEG)
    new_stab = jnp.maximum(old_log, jnp.max(keep_log, axis=-1))
    scaled = jnp.exp(keep_log - new_stab[:, None])
    decayed = jnp.exp(old_log - new_stab)
    memory = decayed[:, None, None] * memory + jnp.einsum(
        "hs,hsd,hse->hde", scaled, k_blk, v_blk, precision=HIGH
    )
    normer = decayed[:, None] * normer + jnp.einsum("hs,hsd->hd", scaled, k_blk, precision=HIGH)
    return ((memory, normer, new_stab, end_doc), (numerator, denominator, peak_log, cumulative))


def split_heads(source, blocks):
    return source.astype(jnp.float32).reshape(blocks, BLOCK, -1, DH).transpose(0, 2, 1, 3)


def split_gates(source, blocks):
    return source.reshape(blocks, BLOCK, -1).transpose(0, 2, 1)


def within_block_pass(
    queries, keys, values, input_gate_log, forget_gate_logits, extra_decay_log, document
):
    blocks = queries.shape[0] // BLOCK
    head_count = queries.shape[1] // DH
    query_heads = split_heads(queries, blocks) * DH ** (-0.5)
    forget_log_values = jax.nn.log_sigmoid(forget_gate_logits) + extra_decay_log
    inputs = (
        query_heads,
        split_heads(keys, blocks),
        split_heads(values, blocks),
        split_gates(input_gate_log, blocks),
        split_gates(forget_log_values, blocks),
        document.reshape(blocks, BLOCK),
    )
    initial = (
        jnp.zeros((head_count, DH, DH), jnp.float32),
        jnp.zeros((head_count, DH), jnp.float32),
        jnp.full((head_count,), NEG, jnp.float32),
        jnp.array(-1, jnp.int32),
    )
    final_state, output_rows = lax.scan(block_terms, initial, inputs)
    return (query_heads, final_state, output_rows)


def head_mix(cell_out, output_gate_logits, cell_norm_gain):
    row_count = output_gate_logits.shape[0]
    head_count = cell_out.shape[1]
    hidden = cell_out.transpose(0, 2, 1, 3).reshape(row_count, head_count * DH)
    squares = lax.psum(jnp.sum(hidden * hidden, axis=1), "tp")
    inverse = lax.rsqrt(squares / (head_count * DH * lax.axis_size("tp")) + EPS)
    gated = jax.nn.sigmoid(output_gate_logits.astype(jnp.float32))
    gains = cell_norm_gain.astype(jnp.float32)
    return (gated * hidden * inverse[:, None] * gains[None, :]).astype(jnp.bfloat16)


def join_states(earlier, later):
    mem_a, norm_a, stab_a, log_a, first_a, last_a = earlier
    mem_b, norm_b, stab_b, log_b, first_b, last_b = later
    joined = last_a == last_b
    stab_ab = jnp.where(joined, jnp.maximum(log_b + stab_a, stab_b), stab_b)
    weight_a = jnp.where(joined, jnp.exp(log_b + stab_a - stab_ab), 0.0)
    weight_b = jnp.exp(stab_b - stab_ab)
    memory = weight_a[:, None, None] * mem_a + weight_b[:, None, None] * mem_b
    normer = weight_a[:, None] * norm_a + weight_b[:, None] * norm_b
    blank_b = last_b < 0
    memory = jnp.where(blank_b, mem_a, memory)
    normer = jnp.where(blank_b, norm_a, normer)
    stabil = jnp.where(blank_b, stab_a, stab_ab)
    first_doc = jnp.where(first_a < 0, first_b, first_a)
    last_doc = jnp.where(blank_b, last_a, last_b)
    return (memory, normer, stabil, log_a + log_b, first_doc, last_doc)


def local(
    queries,
    keys,
    values,
    output_gate_logits,
    input_gate_log,
    forget_gate_logits,
    extra_decay_log,
    document,
    residual,
    cell_norm_gain,
    output_weight,
    mixer_norm_gain,
    up_weight,
    down_weight,
):
    query_heads, final_state, output_rows = within_block_pass(
        queries, keys, values, input_gate_log, forget_gate_logits, extra_decay_log, document
    )
    numerator, denominator, peak_log, cumulative = output_rows
    memory, normer, stabil, last_doc = final_state
    step_logs = cumulative[:, :, -1]
    offsets = jnp.cumsum(step_logs, axis=0) - step_logs
    through = cumulative + offsets[:, :, None]
    summary = (memory, normer, stabil, jnp.sum(step_logs, axis=0), document[0], last_doc)
    identity = (
        jnp.zeros_like(memory),
        jnp.zeros_like(normer),
        jnp.full_like(stabil, NEG),
        jnp.zeros_like(stabil),
        jnp.array(-1, jnp.int32),
        jnp.array(-1, jnp.int32),
    )
    prefix = carried_in(summary, "sp", join_states, identity)
    doc_blocks = document.reshape(-1, BLOCK)
    carried_log = jnp.where(
        (doc_blocks == prefix[5])[:, None, :], through + prefix[2][None, :, None], NEG
    )
    merged_peak = jnp.maximum(peak_log, carried_log)
    own_weight = jnp.exp(peak_log - merged_peak)
    far_weight = jnp.exp(carried_log - merged_peak)
    numerator = own_weight[..., None] * numerator + far_weight[..., None] * jnp.einsum(
        "nhtd,hde->nhte", query_heads, prefix[0], precision=HIGH
    )
    denominator = own_weight * denominator + far_weight * jnp.einsum(
        "nhtd,hd->nht", query_heads, prefix[1], precision=HIGH
    )
    cell_out = numerator / jnp.maximum(jnp.abs(denominator), 1.0)[..., None]
    mixed = head_mix(cell_out, output_gate_logits, cell_norm_gain)
    head_terms = jnp.dot(mixed, output_weight, preferred_element_type=jnp.float32)
    width = residual.shape[1]
    model_width = width * lax.axis_size("tp")
    own_sum = lax.psum_scatter(
        head_terms.astype(jnp.bfloat16), "tp", scatter_dimension=1, tiled=True
    ).astype(jnp.float32)
    first_sum = (residual.astype(jnp.float32) + own_sum).astype(jnp.bfloat16)
    first_wide = lax.optimization_barrier(first_sum).astype(jnp.float32)
    squares = lax.psum(jnp.sum(first_wide * first_wide, axis=1), "tp")
    inverse = lax.rsqrt(squares / model_width + EPS)
    normed_own = (first_wide * inverse[:, None] * mixer_norm_gain.astype(jnp.float32)).astype(
        jnp.bfloat16
    )
    normed_full = lax.all_gather(normed_own, "tp", axis=1, tiled=True)
    hidden = jnp.dot(
        normed_full,
        lax.all_gather(up_weight, "sp", axis=0, tiled=True),
        preferred_element_type=jnp.float32,
    )
    squared = jnp.square(jax.nn.relu(hidden)).astype(jnp.bfloat16)
    channel = jnp.dot(
        squared,
        lax.all_gather(down_weight, "sp", axis=1, tiled=True),
        preferred_element_type=jnp.float32,
    )
    own_channel = lax.psum_scatter(
        channel.astype(jnp.bfloat16), "tp", scatter_dimension=1, tiled=True
    ).astype(jnp.float32)
    return (lax.optimization_barrier(first_sum).astype(jnp.float32) + own_channel).astype(
        jnp.bfloat16
    )


MESH = pl.DeviceIdType.MESH
F32 = jnp.float32
BF16 = jnp.bfloat16


def to_columns(rows):
    pad = jnp.zeros((128 - rows.shape[0], rows.shape[1]), F32)
    return jnp.transpose(jnp.concatenate([rows, pad], axis=0))


def row_sums(wide):
    ones = jnp.ones((8, wide.shape[1]), F32)
    return lax.dot_general(
        ones, wide, (((1,), (1,)), ((), ())), precision=HIGH, preferred_element_type=F32
    )


def layer_kernel(
    n,
    m,
    back,
    q_ref,
    k_ref,
    v_ref,
    og_ref,
    gates_ref,
    resid_ref,
    gain_ref,
    wout_ref,
    up_ref,
    down_ref,
    out_ref,
    up_all,
    down_all,
    state_out,
    state_in,
    tail_out,
    tail_in,
    y_ref,
    terms_out,
    terms_in,
    squares_out,
    squares_in,
    first_ref,
    normed,
    sums_out,
    sums_in,
    squared,
    parts_out,
    parts_in,
    ring_send,
    ring_recv,
    state_send,
    state_recv,
    tail_send,
    tail_recv,
    terms_send,
    terms_recv,
    squares_send,
    squares_recv,
    normed_send,
    normed_recv,
    sums_send,
    sums_recv,
    parts_send,
    parts_recv,
):
    sp, tp = lax.axis_index("sp"), lax.axis_index("tp")
    rows, heads = q_ref.shape[0], q_ref.shape[1] // DH
    depth, hidden_width = up_ref.shape
    half, quarter = depth // 2, depth // 4
    width = resid_ref.shape[1]
    per_owner = width // depth

    def index_of(position):
        late = position // (n // 2)
        return (1 - late) * 2 * position + late * (2 * (n - 1 - position) + 1)

    odd = sp % 2
    place = (1 - odd) * (sp // 2) + odd * (n - 1 - sp // 2)
    target = (index_of((place + 1) % n), index_of((place + n - 1) % n))

    barrier = pltpu.get_barrier_semaphore()
    for k in range(1, n):
        pl.semaphore_signal(barrier, device_id=((sp + k) % n, tp), device_id_type=MESH)
    for k in range(1, m):
        pl.semaphore_signal(barrier, device_id=(sp, (tp + k) % m), device_id_type=MESH)
    pl.semaphore_wait(barrier, n + m - 2)

    def block_at(way, step):
        return index_of((place + (n - step if way == 0 else step)) % n)

    def ring(stream, way, step, sub):
        block = block_at(way, step)
        if stream == 0:
            inner = way * half + sub * quarter
            where = pl.ds(pl.multiple_of(block * depth + inner, quarter), quarter)
            dst = up_all.at[where, :]
            src = up_ref.at[pl.ds(inner, quarter), :] if step == 0 else dst
        else:
            deep = pl.ds(sub * (hidden_width // 2), hidden_width // 2)
            dst = down_all.at[block, way, deep, :]
            src = down_ref.at[deep, pl.ds(way * half, half)] if step == 0 else dst
        return pltpu.make_async_remote_copy(
            src_ref=src,
            dst_ref=dst,
            send_sem=ring_send.at[stream, way, step, sub],
            recv_sem=ring_recv.at[stream, way, step, sub],
            device_id=(target[way], tp),
            device_id_type=MESH,
        )

    def arrived(stream, way, step, sub):
        block = block_at(way, step + 1)
        if stream == 0:
            inner = way * half + sub * quarter
            dst = up_all.at[pl.ds(pl.multiple_of(block * depth + inner, quarter), quarter), :]
        else:
            dst = down_all.at[block, way, pl.ds(sub * (hidden_width // 2), hidden_width // 2), :]
        pltpu.make_async_remote_copy(
            src_ref=dst,
            dst_ref=dst,
            send_sem=ring_send.at[stream, way, step, sub],
            recv_sem=ring_recv.at[stream, way, step, sub],
            device_id=(target[way], tp),
            device_id_type=MESH,
        ).wait_recv()

    def open_stream(stream, sub):
        for way in range(2):
            ring(stream, way, 0, sub).start()

    events = [(a, b, c) for a in range(2) for b in range(n - 1) for c in range(2)]
    done = [0]

    def pump():
        stream, step, sub = events[done[0]]
        done[0] += 1
        for way in range(2):
            arrived(stream, way, step, sub)
            if step + 1 < n - 1:
                ring(stream, way, step + 1, sub).start()
        if stream == 0 and step == n - 2:
            open_stream(1, sub)

    open_stream(0, 0)

    gates = gates_ref[...]
    document = gates[2 * heads : 2 * heads + 1, :]
    across = lax.broadcasted_iota(jnp.int32, (rows, rows), 1)
    along = lax.broadcasted_iota(jnp.int32, (rows, rows), 0)
    upper = (along <= across).astype(F32)
    sums = jnp.dot(gates, upper, precision=HIGH, preferred_element_type=F32)
    last_doc = document[:, rows - 1 : rows]
    totals, stabs, scaled = [], [], []
    for h in range(heads):
        total = sums[h : h + 1, rows - 1 : rows]
        keep = total - sums[h : h + 1, :] + gates[heads + h : heads + h + 1, :]
        keep = jnp.where(document == last_doc, keep, NEG)
        stab = jnp.max(keep, axis=1, keepdims=True)
        totals.append(total)
        stabs.append(stab)
        scaled.append(jnp.exp(keep - stab))
    slab = lax.broadcasted_iota(jnp.int32, (8, rows), 0)
    packed = jnp.broadcast_to(document, (8, rows))
    for h in range(heads):
        packed = jnp.where(slab == h, sums[h : h + 1, :], packed)
        packed = jnp.where(slab == heads + h, scaled[h], packed)
    columns = to_columns(packed)
    doc_col = columns[:, 2 * heads : 2 * heads + 1]
    line = lax.broadcasted_iota(jnp.int32, (8, DH), 0)
    for h in range(heads):
        mine = slice(h * DH, (h + 1) * DH)
        weighted = k_ref[:, mine].astype(F32) * columns[:, heads + h : heads + h + 1]
        state_out[h] = jnp.dot(
            jnp.transpose(weighted),
            v_ref[:, mine].astype(F32),
            precision=HIGH,
            preferred_element_type=F32,
        ).astype(BF16)
        tail = jnp.broadcast_to(jnp.sum(weighted, axis=0, keepdims=True), (8, DH))
        tail = jnp.where(line == 1, stabs[h], tail)
        tail = jnp.where(line == 2, totals[h], tail)
        tail = jnp.where(line == 3, last_doc, tail)
        tail_out[h] = tail

    def state_copies(k):
        return [
            pltpu.make_async_remote_copy(
                src_ref=src,
                dst_ref=dst.at[k - 1],
                send_sem=send_sem.at[k - 1],
                recv_sem=recv_sem.at[k - 1],
                device_id=((sp + k) % n, tp),
                device_id_type=MESH,
            )
            for src, dst, send_sem, recv_sem in (
                (tail_out, tail_in, tail_send, tail_recv),
                (state_out, state_in, state_send, state_recv),
            )
        ]

    for k in range(1, back + 1):

        @pl.when(sp + k < n)
        def _():
            for copy in state_copies(k):
                copy.start()

        @pl.when(sp < k)
        def _():
            tail_in[k - 1] = jnp.zeros((heads, 8, DH), F32)
            state_in[k - 1] = jnp.zeros((heads, DH, DH), BF16)

    open_stream(0, 1)

    own_rows = pl.ds(pl.multiple_of(sp * depth, depth), depth)
    up_all[own_rows, :] = up_ref[...]
    down_all[sp, 0] = down_ref[:, 0:half]
    down_all[sp, 1] = down_ref[:, half:depth]
    pump()

    locals_of = []
    for h in range(heads):
        mine = slice(h * DH, (h + 1) * DH)
        scores = lax.dot_general(
            q_ref[:, mine],
            k_ref[:, mine],
            (((1,), (1,)), ((), ())),
            preferred_element_type=F32,
        ) * (DH**-0.5)
        pair = columns[:, h : h + 1] - sums[h : h + 1, :] + gates[heads + h : heads + h + 1, :]
        pair = jnp.where((doc_col == document) & (along >= across), pair, NEG)
        peak = jnp.max(pair, axis=1, keepdims=True)
        scores = scores * jnp.exp(pair - peak)
        numer = jnp.dot(
            scores, v_ref[:, mine].astype(F32), precision=HIGH, preferred_element_type=F32
        )
        locals_of.append((peak, jnp.sum(scores, axis=1, keepdims=True), numer))
        pump()

    for k in range(1, back + 1):

        @pl.when(sp >= k)
        def _():
            for copy in state_copies(k):
                copy.wait_recv()

    first_doc = document[:, 0:1]
    cells = []
    for h in range(heads):
        mine = slice(h * DH, (h + 1) * DH)
        between = jnp.zeros((1, DH), F32)
        logs, valids = [], []
        best = jnp.full((1, DH), NEG, F32)
        for k in range(1, back + 1):
            tail = tail_in[k - 1, h]
            far = lax.broadcasted_iota(jnp.int32, (1, DH), 1) * 0 + sp
            valid = (tail[3:4, :] == first_doc) & (far >= k)
            log = jnp.where(valid, between + tail[1:2, :], NEG)
            between = between + tail[2:3, :]
            best = jnp.maximum(best, log)
            logs.append(log)
            valids.append(valid)
        memory = jnp.zeros((DH, DH), F32)
        normer = jnp.zeros((1, DH), F32)
        for k in range(1, back + 1):
            weight = jnp.where(valids[k - 1], jnp.exp(logs[k - 1] - best), 0.0)
            memory = memory + jnp.where(
                valids[k - 1], weight * state_in[k - 1, h].astype(F32), 0.0
            )
            normer = normer + jnp.where(
                valids[k - 1], weight * tail_in[k - 1, h, 0:1, :], 0.0
            )
        peak, denom, numer = locals_of[h]
        carried = jnp.where(doc_col == first_doc, columns[:, h : h + 1] + best[:, 0:1], NEG)
        merged = jnp.maximum(peak, carried)
        own, other = jnp.exp(peak - merged), jnp.exp(carried - merged)
        query = q_ref[:, mine].astype(F32) * (DH**-0.5)
        numer = own * numer + other * jnp.dot(
            query, memory, precision=HIGH, preferred_element_type=F32
        )
        denom = own * denom + other * jnp.sum(query * normer, axis=1, keepdims=True)
        cell = numer / jnp.maximum(jnp.abs(denom), 1.0)
        cells.append(cell)
        gated = jax.nn.sigmoid(og_ref[:, mine].astype(F32))
        y_ref[:, mine] = (gated * cell * gain_ref[:, mine].astype(F32)).astype(BF16)
    total = cells[0] * cells[0]
    for h in range(1, heads):
        total = total + cells[h] * cells[h]
    squares_out[...] = row_sums(total)

    def to_peer(src, dst, send_sem, recv_sem, k):
        return pltpu.make_async_remote_copy(
            src_ref=src,
            dst_ref=dst,
            send_sem=send_sem.at[k - 1],
            recv_sem=recv_sem.at[k - 1],
            device_id=(sp, (tp + k) % m),
            device_id_type=MESH,
        )

    def squares_copy(k):
        return to_peer(squares_out, squares_in.at[k - 1], squares_send, squares_recv, k)

    def terms_copy(k):
        return to_peer(terms_out.at[k], terms_in.at[k - 1], terms_send, terms_recv, k)

    def head_term(k):
        owner = (tp + k) % m
        cols = pl.ds(pl.multiple_of(owner * width, width), width)
        return jnp.dot(y_ref[...], wout_ref[:, cols], preferred_element_type=F32).astype(BF16)

    for k in range(1, m):
        squares_copy(k).start()
        terms_out[k] = head_term(k)
        terms_copy(k).start()
    own_term = head_term(0).astype(F32)
    terms_out[0] = own_term.astype(BF16)
    for _ in range(min(PUMPS_TERMS, 2 * (n - 1) - done[0])):
        pump()
    for k in range(1, m):
        squares_copy(k).wait_recv()
        terms_copy(k).wait_recv()
    squares = squares_out[...]
    attn = terms_out[0].astype(F32)
    for k in range(1, m):
        squares = squares + squares_in[k - 1]
        attn = attn + terms_in[k - 1].astype(F32)
    inverse = lax.rsqrt(to_columns(squares)[:, 0:1] / (heads * DH * m) + EPS)
    first = (resid_ref[...].astype(F32) + attn * inverse).astype(BF16)
    first_ref[...] = first
    first = first.astype(F32)
    here = pl.ds(pl.multiple_of(tp * width, width), width)
    normed[:, here] = (first * gain_ref[:, heads * DH :].astype(F32)).astype(BF16)
    sums_out[...] = row_sums(first * first)

    def normed_copy(k):
        return to_peer(normed.at[:, here], normed.at[:, here], normed_send, normed_recv, k)

    def normed_arrival(k):
        source = (tp + m - k) % m
        there = normed.at[:, pl.ds(pl.multiple_of(source * width, width), width)]
        return to_peer(there, there, normed_send, normed_recv, k)

    def sums_copy(k):
        return to_peer(sums_out, sums_in.at[k - 1], sums_send, sums_recv, k)

    for k in range(1, m):
        sums_copy(k).start()
        normed_copy(k).start()
    while done[0] < 2 * (n - 1):
        pump()
    for k in range(1, m):
        sums_copy(k).wait_recv()
        normed_arrival(k).wait_recv()
    squares = sums_out[...]
    for k in range(1, m):
        squares = squares + sums_in[k - 1]
    scale = lax.rsqrt(to_columns(squares)[:, 0:1] / (width * m) + EPS)

    tile = min(hidden_width, 256)
    chunks = hidden_width // tile

    def up_chunk(c, carry):
        cols = pl.ds(pl.multiple_of(c * tile, tile), tile)
        raw = jnp.dot(normed[...], up_all[:, cols], preferred_element_type=F32)
        hidden = jnp.maximum(raw * scale, 0.0)
        squared[:, cols] = (hidden * hidden).astype(BF16)
        return carry

    lax.fori_loop(0, chunks // 2, up_chunk, 0)
    pump()
    lax.fori_loop(chunks // 2, chunks, up_chunk, 0)

    def part_copy(way, step):
        block = block_at(way, step)
        owner, slot = block // per_owner, block % per_owner
        return owner, pltpu.make_async_remote_copy(
            src_ref=parts_out.at[block, way],
            dst_ref=parts_in.at[tp, slot, way],
            send_sem=parts_send.at[block, way],
            recv_sem=parts_recv.at[tp, slot, way],
            device_id=(sp, owner),
            device_id_type=MESH,
        )

    def down_block(step):
        for way in range(2):
            block = block_at(way, step)
            parts_out[block, way] = jnp.dot(
                squared[...], down_all[block, way], preferred_element_type=F32
            ).astype(BF16)
            owner, copy = part_copy(way, step)

            @pl.when(owner != tp)
            def _():
                copy.start()

    down_block(0)
    for step in range(1, n):
        while done[0] < 2 * (n - 1) + 2 * step:
            pump()
        down_block(step)

    for slot in range(per_owner):
        for way in range(2):
            cols = slice(slot * depth + way * half, slot * depth + (way + 1) * half)
            total = parts_out[tp * per_owner + slot, way].astype(F32)
            for k in range(1, m):
                source = (tp + k) % m
                there = parts_in.at[source, slot, way]
                pltpu.make_async_remote_copy(
                    src_ref=there,
                    dst_ref=there,
                    send_sem=parts_send.at[0, 0],
                    recv_sem=parts_recv.at[source, slot, way],
                    device_id=(sp, source),
                    device_id_type=MESH,
                ).wait_recv()
                total = total + parts_in[source, slot, way].astype(F32)
            out_ref[:, cols] = (first_ref[:, cols].astype(F32) + total).astype(BF16)

    for stream, step, sub in events:
        for way in range(2):
            ring(stream, way, step, sub).wait_send()
    for k in range(1, back + 1):

        @pl.when(sp + k < n)
        def _():
            for copy in state_copies(k):
                copy.wait_send()

    for k in range(1, m):
        squares_copy(k).wait_send()
        terms_copy(k).wait_send()
        sums_copy(k).wait_send()
        normed_copy(k).wait_send()
    for step in range(n):
        for way in range(2):
            owner, copy = part_copy(way, step)

            @pl.when(owner != tp)
            def _():
                copy.wait_send()


PUMPS_TERMS = 5


def fused(
    n,
    m,
    queries,
    keys,
    values,
    output_gate_logits,
    input_gate_log,
    forget_gate_logits,
    extra_decay_log,
    document,
    residual,
    cell_norm_gain,
    output_weight,
    mixer_norm_gain,
    up_weight,
    down_weight,
):
    rows, heads = queries.shape[0], queries.shape[1] // DH
    depth, hidden_width = up_weight.shape
    width = residual.shape[1]
    back = min(n - 1, (MOST - 2) // rows + 1)
    forget = jax.nn.log_sigmoid(forget_gate_logits) + extra_decay_log
    gates = jnp.concatenate(
        [forget.T, input_gate_log.T, document.astype(F32)[None, :]], axis=0
    )
    gates = jnp.pad(gates, ((0, 8 - gates.shape[0]), (0, 0)))
    dma = pltpu.SemaphoreType.DMA
    per_owner = width // depth
    return pl.pallas_call(
        functools.partial(layer_kernel, n, m, back),
        out_shape=jax.ShapeDtypeStruct((rows, width), BF16),
        in_specs=[pl.BlockSpec(memory_space=pltpu.VMEM)] * 10,
        out_specs=pl.BlockSpec(memory_space=pltpu.VMEM),
        scratch_shapes=[
            pltpu.VMEM((n * depth, hidden_width), BF16),
            pltpu.VMEM((n, 2, hidden_width, depth // 2), BF16),
            pltpu.VMEM((heads, DH, DH), BF16),
            pltpu.VMEM((back, heads, DH, DH), BF16),
            pltpu.VMEM((heads, 8, DH), F32),
            pltpu.VMEM((back, heads, 8, DH), F32),
            pltpu.VMEM((rows, heads * DH), BF16),
            pltpu.VMEM((m, rows, width), BF16),
            pltpu.VMEM((m - 1, rows, width), BF16),
            pltpu.VMEM((8, rows), F32),
            pltpu.VMEM((m - 1, 8, rows), F32),
            pltpu.VMEM((rows, width), BF16),
            pltpu.VMEM((rows, m * width), BF16),
            pltpu.VMEM((8, rows), F32),
            pltpu.VMEM((m - 1, 8, rows), F32),
            pltpu.VMEM((rows, hidden_width), BF16),
            pltpu.VMEM((n, 2, rows, depth // 2), BF16),
            pltpu.VMEM((m, per_owner, 2, rows, depth // 2), BF16),
            dma((2, 2, n - 1, 2)),
            dma((2, 2, n - 1, 2)),
            dma((back,)),
            dma((back,)),
            dma((back,)),
            dma((back,)),
            dma((m - 1,)),
            dma((m - 1,)),
            dma((m - 1,)),
            dma((m - 1,)),
            dma((m - 1,)),
            dma((m - 1,)),
            dma((m - 1,)),
            dma((m - 1,)),
            dma((n, 2)),
            dma((m, per_owner, 2)),
        ],
        compiler_params=pltpu.CompilerParams(
            collective_id=0, has_side_effects=True, vmem_limit_bytes=60 * 1024 * 1024
        ),
        name="layer",
    )(
        queries,
        keys,
        values,
        output_gate_logits,
        gates,
        residual,
        jnp.concatenate([cell_norm_gain, mixer_norm_gain])[None, :],
        output_weight,
        up_weight,
        down_weight,
    )


def either(n, m, *args):
    depth, hidden_width = args[12].shape
    heads = args[0].shape[1] // DH
    fits = depth % 256 == 0 and n % 2 == 0 and n >= 4 and n <= 16 and m >= 2
    fits = fits and 2 * heads + 1 <= 8 and args[8].shape[1] % depth == 0
    fits = fits and args[0].shape[0] % 128 == 0 and hidden_width % 256 == 0
    if fits:
        return fused(n, m, *args)
    return local(*args)


def solution(mesh):
    in_specs = (
        P("sp", "tp"),
        P("sp", "tp"),
        P("sp", "tp"),
        P("sp", "tp"),
        P("sp", "tp"),
        P("sp", "tp"),
        P("sp", "tp"),
        P("sp"),
        P("sp", "tp"),
        P("tp"),
        P("tp", None),
        P("tp"),
        P("sp", "tp"),
        P("tp", "sp"),
    )
    out_specs = P("sp", "tp")
    body = functools.partial(either, mesh.shape["sp"], mesh.shape["tp"])
    return jax.shard_map(body, mesh=mesh, in_specs=in_specs, out_specs=out_specs, check_vma=False)
```

```python
import functools

import jax
import jax.numpy as jnp
from jax import lax
from jax.experimental import pallas as pl
from jax.experimental.pallas import tpu as pltpu
from jax.sharding import PartitionSpec as P

DH = 128
BLOCK = 128
MOST = 2048


NEG = -1e30
EPS = 1e-06
HIGH = lax.Precision.HIGHEST


def carried_in(value, axis, join, neutral):
    count, mine = (lax.axis_size(axis), lax.axis_index(axis))
    pieces = jax.tree.map(lambda part: lax.all_gather(part, axis), value)
    subtotal = jax.tree.map(
        lambda part, zero: jnp.full_like(part, 0) + jnp.asarray(zero, part.dtype), value, neutral
    )

    def step(position, subtotal):
        longer = join(subtotal, jax.tree.map(lambda part: part[position], pieces))
        return jax.tree.map(lambda new, old: jnp.where(position < mine, new, old), longer, subtotal)

    return lax.fori_loop(0, count - 1, step, subtotal)


def block_terms(carry, inputs):
    memory, normer, stabil, last_doc = carry
    q_blk, k_blk, v_blk, gate_in, gate_log, doc_blk = inputs
    length = doc_blk.shape[0]
    causal = jnp.arange(length)[:, None] >= jnp.arange(length)[None, :]
    cumulative = jnp.cumsum(gate_log, axis=-1)
    same_doc = (doc_blk[:, None] == doc_blk[None, :]) & causal
    pair_log = cumulative[:, :, None] - cumulative[:, None, :] + gate_in[:, None, :]
    pair_log = jnp.where(same_doc[None], pair_log, NEG)
    live_rows = doc_blk == last_doc
    carried_log = jnp.where(live_rows[None, :], cumulative + stabil[:, None], NEG)
    peak_log = jnp.maximum(carried_log, jnp.max(pair_log, axis=-1))
    weights = jnp.exp(pair_log - peak_log[:, :, None])
    carried = jnp.exp(carried_log - peak_log)
    scores = jnp.einsum("htd,hsd->hts", q_blk, k_blk, precision=HIGH) * weights
    numerator = carried[:, :, None] * jnp.einsum("htd,hde->hte", q_blk, memory, precision=HIGH)
    numerator = numerator + jnp.einsum("hts,hse->hte", scores, v_blk, precision=HIGH)
    denominator = carried * jnp.einsum("htd,hd->ht", q_blk, normer, precision=HIGH) + jnp.sum(
        scores, axis=-1
    )
    end_doc = doc_blk[-1]
    end_cum = cumulative[:, -1]
    keep_log = jnp.where(
        (doc_blk == end_doc)[None, :], end_cum[:, None] - cumulative + gate_in, NEG
    )
    old_log = jnp.where(last_doc == end_doc, end_cum + stabil, NEG)
    new_stab = jnp.maximum(old_log, jnp.max(keep_log, axis=-1))
    scaled = jnp.exp(keep_log - new_stab[:, None])
    decayed = jnp.exp(old_log - new_stab)
    memory = decayed[:, None, None] * memory + jnp.einsum(
        "hs,hsd,hse->hde", scaled, k_blk, v_blk, precision=HIGH
    )
    normer = decayed[:, None] * normer + jnp.einsum("hs,hsd->hd", scaled, k_blk, precision=HIGH)
    return ((memory, normer, new_stab, end_doc), (numerator, denominator, peak_log, cumulative))


def split_heads(source, blocks):
    return source.astype(jnp.float32).reshape(blocks, BLOCK, -1, DH).transpose(0, 2, 1, 3)


def split_gates(source, blocks):
    return source.reshape(blocks, BLOCK, -1).transpose(0, 2, 1)


def within_block_pass(
    queries, keys, values, input_gate_log, forget_gate_logits, extra_decay_log, document
):
    blocks = queries.shape[0] // BLOCK
    head_count = queries.shape[1] // DH
    query_heads = split_heads(queries, blocks) * DH ** (-0.5)
    forget_log_values = jax.nn.log_sigmoid(forget_gate_logits) + extra_decay_log
    inputs = (
        query_heads,
        split_heads(keys, blocks),
        split_heads(values, blocks),
        split_gates(input_gate_log, blocks),
        split_gates(forget_log_values, blocks),
        document.reshape(blocks, BLOCK),
    )
    initial = (
        jnp.zeros((head_count, DH, DH), jnp.float32),
        jnp.zeros((head_count, DH), jnp.float32),
        jnp.full((head_count,), NEG, jnp.float32),
        jnp.array(-1, jnp.int32),
    )
    final_state, output_rows = lax.scan(block_terms, initial, inputs)
    return (query_heads, final_state, output_rows)


def head_mix(cell_out, output_gate_logits, cell_norm_gain):
    row_count = output_gate_logits.shape[0]
    head_count = cell_out.shape[1]
    hidden = cell_out.transpose(0, 2, 1, 3).reshape(row_count, head_count * DH)
    squares = lax.psum(jnp.sum(hidden * hidden, axis=1), "tp")
    inverse = lax.rsqrt(squares / (head_count * DH * lax.axis_size("tp")) + EPS)
    gated = jax.nn.sigmoid(output_gate_logits.astype(jnp.float32))
    gains = cell_norm_gain.astype(jnp.float32)
    return (gated * hidden * inverse[:, None] * gains[None, :]).astype(jnp.bfloat16)


def join_states(earlier, later):
    mem_a, norm_a, stab_a, log_a, first_a, last_a = earlier
    mem_b, norm_b, stab_b, log_b, first_b, last_b = later
    joined = last_a == last_b
    stab_ab = jnp.where(joined, jnp.maximum(log_b + stab_a, stab_b), stab_b)
    weight_a = jnp.where(joined, jnp.exp(log_b + stab_a - stab_ab), 0.0)
    weight_b = jnp.exp(stab_b - stab_ab)
    memory = weight_a[:, None, None] * mem_a + weight_b[:, None, None] * mem_b
    normer = weight_a[:, None] * norm_a + weight_b[:, None] * norm_b
    blank_b = last_b < 0
    memory = jnp.where(blank_b, mem_a, memory)
    normer = jnp.where(blank_b, norm_a, normer)
    stabil = jnp.where(blank_b, stab_a, stab_ab)
    first_doc = jnp.where(first_a < 0, first_b, first_a)
    last_doc = jnp.where(blank_b, last_a, last_b)
    return (memory, normer, stabil, log_a + log_b, first_doc, last_doc)


def local(
    queries,
    keys,
    values,
    output_gate_logits,
    input_gate_log,
    forget_gate_logits,
    extra_decay_log,
    document,
    residual,
    cell_norm_gain,
    output_weight,
    mixer_norm_gain,
    up_weight,
    down_weight,
):
    query_heads, final_state, output_rows = within_block_pass(
        queries, keys, values, input_gate_log, forget_gate_logits, extra_decay_log, document
    )
    numerator, denominator, peak_log, cumulative = output_rows
    memory, normer, stabil, last_doc = final_state
    step_logs = cumulative[:, :, -1]
    offsets = jnp.cumsum(step_logs, axis=0) - step_logs
    through = cumulative + offsets[:, :, None]
    summary = (memory, normer, stabil, jnp.sum(step_logs, axis=0), document[0], last_doc)
    identity = (
        jnp.zeros_like(memory),
        jnp.zeros_like(normer),
        jnp.full_like(stabil, NEG),
        jnp.zeros_like(stabil),
        jnp.array(-1, jnp.int32),
        jnp.array(-1, jnp.int32),
    )
    prefix = carried_in(summary, "sp", join_states, identity)
    doc_blocks = document.reshape(-1, BLOCK)
    carried_log = jnp.where(
        (doc_blocks == prefix[5])[:, None, :], through + prefix[2][None, :, None], NEG
    )
    merged_peak = jnp.maximum(peak_log, carried_log)
    own_weight = jnp.exp(peak_log - merged_peak)
    far_weight = jnp.exp(carried_log - merged_peak)
    numerator = own_weight[..., None] * numerator + far_weight[..., None] * jnp.einsum(
        "nhtd,hde->nhte", query_heads, prefix[0], precision=HIGH
    )
    denominator = own_weight * denominator + far_weight * jnp.einsum(
        "nhtd,hd->nht", query_heads, prefix[1], precision=HIGH
    )
    cell_out = numerator / jnp.maximum(jnp.abs(denominator), 1.0)[..., None]
    mixed = head_mix(cell_out, output_gate_logits, cell_norm_gain)
    head_terms = jnp.dot(mixed, output_weight, preferred_element_type=jnp.float32)
    width = residual.shape[1]
    model_width = width * lax.axis_size("tp")
    own_sum = lax.psum_scatter(
        head_terms.astype(jnp.bfloat16), "tp", scatter_dimension=1, tiled=True
    ).astype(jnp.float32)
    first_sum = (residual.astype(jnp.float32) + own_sum).astype(jnp.bfloat16)
    first_wide = lax.optimization_barrier(first_sum).astype(jnp.float32)
    squares = lax.psum(jnp.sum(first_wide * first_wide, axis=1), "tp")
    inverse = lax.rsqrt(squares / model_width + EPS)
    normed_own = (first_wide * inverse[:, None] * mixer_norm_gain.astype(jnp.float32)).astype(
        jnp.bfloat16
    )
    normed_full = lax.all_gather(normed_own, "tp", axis=1, tiled=True)
    hidden = jnp.dot(
        normed_full,
        lax.all_gather(up_weight, "sp", axis=0, tiled=True),
        preferred_element_type=jnp.float32,
    )
    squared = jnp.square(jax.nn.relu(hidden)).astype(jnp.bfloat16)
    channel = jnp.dot(
        squared,
        lax.all_gather(down_weight, "sp", axis=1, tiled=True),
        preferred_element_type=jnp.float32,
    )
    own_channel = lax.psum_scatter(
        channel.astype(jnp.bfloat16), "tp", scatter_dimension=1, tiled=True
    ).astype(jnp.float32)
    return (lax.optimization_barrier(first_sum).astype(jnp.float32) + own_channel).astype(
        jnp.bfloat16
    )


MESH = pl.DeviceIdType.MESH
F32 = jnp.float32
BF16 = jnp.bfloat16


def to_columns(rows):
    pad = jnp.zeros((128 - rows.shape[0], rows.shape[1]), F32)
    return jnp.transpose(jnp.concatenate([rows, pad], axis=0))


def row_sums(wide):
    ones = jnp.ones((8, wide.shape[1]), F32)
    return lax.dot_general(
        ones, wide, (((1,), (1,)), ((), ())), precision=HIGH, preferred_element_type=F32
    )


def layer_kernel(
    n,
    m,
    back,
    q_ref,
    k_ref,
    v_ref,
    og_ref,
    gates_ref,
    resid_ref,
    gain_ref,
    wout_ref,
    up_ref,
    down_ref,
    out_ref,
    up_all,
    down_all,
    state_out,
    state_in,
    tail_out,
    tail_in,
    y_ref,
    terms_out,
    terms_in,
    squares_out,
    squares_in,
    first_ref,
    normed,
    sums_out,
    sums_in,
    squared,
    parts_out,
    parts_in,
    ring_send,
    ring_recv,
    state_send,
    state_recv,
    tail_send,
    tail_recv,
    terms_send,
    terms_recv,
    squares_send,
    squares_recv,
    normed_send,
    normed_recv,
    sums_send,
    sums_recv,
    parts_send,
    parts_recv,
):
    sp, tp = lax.axis_index("sp"), lax.axis_index("tp")
    rows, heads = q_ref.shape[0], q_ref.shape[1] // DH
    depth, hidden_width = up_ref.shape
    half, quarter = depth // 2, depth // 4
    width = resid_ref.shape[1]
    per_owner = width // depth

    def index_of(position):
        late = position // (n // 2)
        return (1 - late) * 2 * position + late * (2 * (n - 1 - position) + 1)

    odd = sp % 2
    place = (1 - odd) * (sp // 2) + odd * (n - 1 - sp // 2)
    target = (index_of((place + 1) % n), index_of((place + n - 1) % n))

    barrier = pltpu.get_barrier_semaphore()
    for k in range(1, n):
        pl.semaphore_signal(barrier, device_id=((sp + k) % n, tp), device_id_type=MESH)
    for k in range(1, m):
        pl.semaphore_signal(barrier, device_id=(sp, (tp + k) % m), device_id_type=MESH)
    pl.semaphore_wait(barrier, n + m - 2)

    def block_at(way, step):
        return index_of((place + (n - step if way == 0 else step)) % n)

    def ring(stream, way, step, sub):
        block = block_at(way, step)
        if stream == 0:
            inner = way * half + sub * quarter
            where = pl.ds(pl.multiple_of(block * depth + inner, quarter), quarter)
            dst = up_all.at[where, :]
            src = up_ref.at[pl.ds(inner, quarter), :] if step == 0 else dst
        else:
            deep = pl.ds(sub * (hidden_width // 2), hidden_width // 2)
            dst = down_all.at[block, way, deep, :]
            src = down_ref.at[deep, pl.ds(way * half, half)] if step == 0 else dst
        return pltpu.make_async_remote_copy(
            src_ref=src,
            dst_ref=dst,
            send_sem=ring_send.at[stream, way, step, sub],
            recv_sem=ring_recv.at[stream, way, step, sub],
            device_id=(target[way], tp),
            device_id_type=MESH,
        )

    def arrived(stream, way, step, sub):
        block = block_at(way, step + 1)
        if stream == 0:
            inner = way * half + sub * quarter
            dst = up_all.at[pl.ds(pl.multiple_of(block * depth + inner, quarter), quarter), :]
        else:
            dst = down_all.at[block, way, pl.ds(sub * (hidden_width // 2), hidden_width // 2), :]
        pltpu.make_async_remote_copy(
            src_ref=dst,
            dst_ref=dst,
            send_sem=ring_send.at[stream, way, step, sub],
            recv_sem=ring_recv.at[stream, way, step, sub],
            device_id=(target[way], tp),
            device_id_type=MESH,
        ).wait_recv()

    def open_stream(stream, sub):
        for way in range(2):
            ring(stream, way, 0, sub).start()

    events = [(a, b, c) for a in range(2) for b in range(n - 1) for c in range(2)]
    done = [0]

    def pump():
        stream, step, sub = events[done[0]]
        done[0] += 1
        for way in range(2):
            arrived(stream, way, step, sub)
            if step + 1 < n - 1:
                ring(stream, way, step + 1, sub).start()
        if stream == 0 and step == n - 2:
            open_stream(1, sub)

    open_stream(0, 0)

    gates = gates_ref[...]
    document = gates[2 * heads : 2 * heads + 1, :]
    across = lax.broadcasted_iota(jnp.int32, (rows, rows), 1)
    along = lax.broadcasted_iota(jnp.int32, (rows, rows), 0)
    upper = (along <= across).astype(F32)
    sums = jnp.dot(gates, upper, precision=HIGH, preferred_element_type=F32)
    last_doc = document[:, rows - 1 : rows]
    totals, stabs, scaled = [], [], []
    for h in range(heads):
        total = sums[h : h + 1, rows - 1 : rows]
        keep = total - sums[h : h + 1, :] + gates[heads + h : heads + h + 1, :]
        keep = jnp.where(document == last_doc, keep, NEG)
        stab = jnp.max(keep, axis=1, keepdims=True)
        totals.append(total)
        stabs.append(stab)
        scaled.append(jnp.exp(keep - stab))
    slab = lax.broadcasted_iota(jnp.int32, (8, rows), 0)
    packed = jnp.broadcast_to(document, (8, rows))
    for h in range(heads):
        packed = jnp.where(slab == h, sums[h : h + 1, :], packed)
        packed = jnp.where(slab == heads + h, scaled[h], packed)
    columns = to_columns(packed)
    doc_col = columns[:, 2 * heads : 2 * heads + 1]
    line = lax.broadcasted_iota(jnp.int32, (8, DH), 0)
    for h in range(heads):
        mine = slice(h * DH, (h + 1) * DH)
        weighted = k_ref[:, mine].astype(F32) * columns[:, heads + h : heads + h + 1]
        state_out[h] = jnp.dot(
            jnp.transpose(weighted),
            v_ref[:, mine].astype(F32),
            precision=HIGH,
            preferred_element_type=F32,
        ).astype(BF16)
        tail = jnp.broadcast_to(jnp.sum(weighted, axis=0, keepdims=True), (8, DH))
        tail = jnp.where(line == 1, stabs[h], tail)
        tail = jnp.where(line == 2, totals[h], tail)
        tail = jnp.where(line == 3, last_doc, tail)
        tail_out[h] = tail

    def state_copies(k):
        return [
            pltpu.make_async_remote_copy(
                src_ref=src,
                dst_ref=dst.at[k - 1],
                send_sem=send_sem.at[k - 1],
                recv_sem=recv_sem.at[k - 1],
                device_id=((sp + k) % n, tp),
                device_id_type=MESH,
            )
            for src, dst, send_sem, recv_sem in (
                (tail_out, tail_in, tail_send, tail_recv),
                (state_out, state_in, state_send, state_recv),
            )
        ]

    for k in range(1, back + 1):

        @pl.when(sp + k < n)
        def _():
            for copy in state_copies(k):
                copy.start()

        @pl.when(sp < k)
        def _():
            tail_in[k - 1] = jnp.zeros((heads, 8, DH), F32)
            state_in[k - 1] = jnp.zeros((heads, DH, DH), BF16)

    open_stream(0, 1)

    own_rows = pl.ds(pl.multiple_of(sp * depth, depth), depth)
    up_all[own_rows, :] = up_ref[...]
    down_all[sp, 0] = down_ref[:, 0:half]
    down_all[sp, 1] = down_ref[:, half:depth]
    pump()

    locals_of = []
    for h in range(heads):
        mine = slice(h * DH, (h + 1) * DH)
        scores = lax.dot_general(
            q_ref[:, mine],
            k_ref[:, mine],
            (((1,), (1,)), ((), ())),
            preferred_element_type=F32,
        ) * (DH**-0.5)
        pair = columns[:, h : h + 1] - sums[h : h + 1, :] + gates[heads + h : heads + h + 1, :]
        pair = jnp.where((doc_col == document) & (along >= across), pair, NEG)
        peak = jnp.max(pair, axis=1, keepdims=True)
        scores = scores * jnp.exp(pair - peak)
        numer = jnp.dot(
            scores, v_ref[:, mine].astype(F32), precision=HIGH, preferred_element_type=F32
        )
        locals_of.append((peak, jnp.sum(scores, axis=1, keepdims=True), numer))
        pump()

    for k in range(1, back + 1):

        @pl.when(sp >= k)
        def _():
            for copy in state_copies(k):
                copy.wait_recv()

    first_doc = document[:, 0:1]
    cells = []
    for h in range(heads):
        mine = slice(h * DH, (h + 1) * DH)
        between = jnp.zeros((1, DH), F32)
        logs, valids = [], []
        best = jnp.full((1, DH), NEG, F32)
        for k in range(1, back + 1):
            tail = tail_in[k - 1, h]
            far = lax.broadcasted_iota(jnp.int32, (1, DH), 1) * 0 + sp
            valid = (tail[3:4, :] == first_doc) & (far >= k)
            log = jnp.where(valid, between + tail[1:2, :], NEG)
            between = between + tail[2:3, :]
            best = jnp.maximum(best, log)
            logs.append(log)
            valids.append(valid)
        memory = jnp.zeros((DH, DH), F32)
        normer = jnp.zeros((1, DH), F32)
        for k in range(1, back + 1):
            weight = jnp.where(valids[k - 1], jnp.exp(logs[k - 1] - best), 0.0)
            memory = memory + jnp.where(
                valids[k - 1], weight * state_in[k - 1, h].astype(F32), 0.0
            )
            normer = normer + jnp.where(
                valids[k - 1], weight * tail_in[k - 1, h, 0:1, :], 0.0
            )
        peak, denom, numer = locals_of[h]
        carried = jnp.where(doc_col == first_doc, columns[:, h : h + 1] + best[:, 0:1], NEG)
        merged = jnp.maximum(peak, carried)
        own, other = jnp.exp(peak - merged), jnp.exp(carried - merged)
        query = q_ref[:, mine].astype(F32) * (DH**-0.5)
        numer = own * numer + other * jnp.dot(
            query, memory, precision=HIGH, preferred_element_type=F32
        )
        denom = own * denom + other * jnp.sum(query * normer, axis=1, keepdims=True)
        cell = numer / jnp.maximum(jnp.abs(denom), 1.0)
        cells.append(cell)
        gated = jax.nn.sigmoid(og_ref[:, mine].astype(F32))
        y_ref[:, mine] = (gated * cell * gain_ref[:, mine].astype(F32)).astype(BF16)
    total = cells[0] * cells[0]
    for h in range(1, heads):
        total = total + cells[h] * cells[h]
    squares_out[...] = row_sums(total)

    def to_peer(src, dst, send_sem, recv_sem, k):
        return pltpu.make_async_remote_copy(
            src_ref=src,
            dst_ref=dst,
            send_sem=send_sem.at[k - 1],
            recv_sem=recv_sem.at[k - 1],
            device_id=(sp, (tp + k) % m),
            device_id_type=MESH,
        )

    def squares_copy(k):
        return to_peer(squares_out, squares_in.at[k - 1], squares_send, squares_recv, k)

    def terms_copy(k):
        return to_peer(terms_out.at[k], terms_in.at[k - 1], terms_send, terms_recv, k)

    def head_term(k):
        owner = (tp + k) % m
        cols = pl.ds(pl.multiple_of(owner * width, width), width)
        return jnp.dot(y_ref[...], wout_ref[:, cols], preferred_element_type=F32).astype(BF16)

    for k in range(1, m):
        squares_copy(k).start()
        terms_out[k] = head_term(k)
        terms_copy(k).start()
    own_term = head_term(0).astype(F32)
    terms_out[0] = own_term.astype(BF16)
    for _ in range(min(PUMPS_TERMS, 2 * (n - 1) - done[0])):
        pump()
    for k in range(1, m):
        squares_copy(k).wait_recv()
        terms_copy(k).wait_recv()
    squares = squares_out[...]
    attn = terms_out[0].astype(F32)
    for k in range(1, m):
        squares = squares + squares_in[k - 1]
        attn = attn + terms_in[k - 1].astype(F32)
    inverse = lax.rsqrt(to_columns(squares)[:, 0:1] / (heads * DH * m) + EPS)
    first = (resid_ref[...].astype(F32) + attn * inverse).astype(BF16)
    first_ref[...] = first
    first = first.astype(F32)
    here = pl.ds(pl.multiple_of(tp * width, width), width)
    normed[:, here] = (first * gain_ref[:, heads * DH :].astype(F32)).astype(BF16)
    sums_out[...] = row_sums(first * first)

    def normed_copy(k):
        return to_peer(normed.at[:, here], normed.at[:, here], normed_send, normed_recv, k)

    def normed_arrival(k):
        source = (tp + m - k) % m
        there = normed.at[:, pl.ds(pl.multiple_of(source * width, width), width)]
        return to_peer(there, there, normed_send, normed_recv, k)

    def sums_copy(k):
        return to_peer(sums_out, sums_in.at[k - 1], sums_send, sums_recv, k)

    for k in range(1, m):
        sums_copy(k).start()
        normed_copy(k).start()
    while done[0] < 2 * (n - 1):
        pump()
    for k in range(1, m):
        sums_copy(k).wait_recv()
        normed_arrival(k).wait_recv()
    squares = sums_out[...]
    for k in range(1, m):
        squares = squares + sums_in[k - 1]
    scale = lax.rsqrt(to_columns(squares)[:, 0:1] / (width * m) + EPS)

    tile = min(hidden_width, 256)
    chunks = hidden_width // tile

    def up_chunk(c, carry):
        cols = pl.ds(pl.multiple_of(c * tile, tile), tile)
        raw = jnp.dot(normed[...], up_all[:, cols], preferred_element_type=F32)
        hidden = jnp.maximum(raw * scale, 0.0)
        squared[:, cols] = (hidden * hidden).astype(BF16)
        return carry

    lax.fori_loop(0, chunks // 2, up_chunk, 0)
    pump()
    lax.fori_loop(chunks // 2, chunks, up_chunk, 0)

    def part_copy(way, step):
        block = block_at(way, step)
        owner, slot = block // per_owner, block % per_owner
        return owner, pltpu.make_async_remote_copy(
            src_ref=parts_out.at[block, way],
            dst_ref=parts_in.at[tp, slot, way],
            send_sem=parts_send.at[block, way],
            recv_sem=parts_recv.at[tp, slot, way],
            device_id=(sp, owner),
            device_id_type=MESH,
        )

    middle = hidden_width // 2

    def part_of(way, step, deep):
        return jnp.dot(
            squared[:, deep],
            down_all[block_at(way, step), way, deep, :],
            preferred_element_type=F32,
        )

    def down_block(step, early=(0.0, 0.0), deep=slice(0, hidden_width)):
        for way in range(2):
            block = block_at(way, step)
            parts_out[block, way] = (early[way] + part_of(way, step, deep)).astype(BF16)
            owner, copy = part_copy(way, step)

            @pl.when(owner != tp)
            def _():
                copy.start()

    down_block(0)
    for step in range(1, n - 1):
        while done[0] < 2 * (n - 1) + 2 * step:
            pump()
        down_block(step)
    pump()
    early = [part_of(way, n - 1, slice(0, middle)) for way in range(2)]
    pump()
    down_block(n - 1, early, slice(middle, hidden_width))

    for slot in range(per_owner):
        for way in range(2):
            cols = slice(slot * depth + way * half, slot * depth + (way + 1) * half)
            total = parts_out[tp * per_owner + slot, way].astype(F32)
            for k in range(1, m):
                source = (tp + k) % m
                there = parts_in.at[source, slot, way]
                pltpu.make_async_remote_copy(
                    src_ref=there,
                    dst_ref=there,
                    send_sem=parts_send.at[0, 0],
                    recv_sem=parts_recv.at[source, slot, way],
                    device_id=(sp, source),
                    device_id_type=MESH,
                ).wait_recv()
                total = total + parts_in[source, slot, way].astype(F32)
            out_ref[:, cols] = (first_ref[:, cols].astype(F32) + total).astype(BF16)

    for stream, step, sub in events:
        for way in range(2):
            ring(stream, way, step, sub).wait_send()
    for k in range(1, back + 1):

        @pl.when(sp + k < n)
        def _():
            for copy in state_copies(k):
                copy.wait_send()

    for k in range(1, m):
        squares_copy(k).wait_send()
        terms_copy(k).wait_send()
        sums_copy(k).wait_send()
        normed_copy(k).wait_send()
    for step in range(n):
        for way in range(2):
            owner, copy = part_copy(way, step)

            @pl.when(owner != tp)
            def _():
                copy.wait_send()


PUMPS_TERMS = 5


def fused(
    n,
    m,
    queries,
    keys,
    values,
    output_gate_logits,
    input_gate_log,
    forget_gate_logits,
    extra_decay_log,
    document,
    residual,
    cell_norm_gain,
    output_weight,
    mixer_norm_gain,
    up_weight,
    down_weight,
):
    rows, heads = queries.shape[0], queries.shape[1] // DH
    depth, hidden_width = up_weight.shape
    width = residual.shape[1]
    back = min(n - 1, (MOST - 2) // rows + 1)
    forget = jax.nn.log_sigmoid(forget_gate_logits) + extra_decay_log
    gates = jnp.concatenate(
        [forget.T, input_gate_log.T, document.astype(F32)[None, :]], axis=0
    )
    gates = jnp.pad(gates, ((0, 8 - gates.shape[0]), (0, 0)))
    dma = pltpu.SemaphoreType.DMA
    per_owner = width // depth
    return pl.pallas_call(
        functools.partial(layer_kernel, n, m, back),
        out_shape=jax.ShapeDtypeStruct((rows, width), BF16),
        in_specs=[pl.BlockSpec(memory_space=pltpu.VMEM)] * 10,
        out_specs=pl.BlockSpec(memory_space=pltpu.VMEM),
        scratch_shapes=[
            pltpu.VMEM((n * depth, hidden_width), BF16),
            pltpu.VMEM((n, 2, hidden_width, depth // 2), BF16),
            pltpu.VMEM((heads, DH, DH), BF16),
            pltpu.VMEM((back, heads, DH, DH), BF16),
            pltpu.VMEM((heads, 8, DH), F32),
            pltpu.VMEM((back, heads, 8, DH), F32),
            pltpu.VMEM((rows, heads * DH), BF16),
            pltpu.VMEM((m, rows, width), BF16),
            pltpu.VMEM((m - 1, rows, width), BF16),
            pltpu.VMEM((8, rows), F32),
            pltpu.VMEM((m - 1, 8, rows), F32),
            pltpu.VMEM((rows, width), BF16),
            pltpu.VMEM((rows, m * width), BF16),
            pltpu.VMEM((8, rows), F32),
            pltpu.VMEM((m - 1, 8, rows), F32),
            pltpu.VMEM((rows, hidden_width), BF16),
            pltpu.VMEM((n, 2, rows, depth // 2), BF16),
            pltpu.VMEM((m, per_owner, 2, rows, depth // 2), BF16),
            dma((2, 2, n - 1, 2)),
            dma((2, 2, n - 1, 2)),
            dma((back,)),
            dma((back,)),
            dma((back,)),
            dma((back,)),
            dma((m - 1,)),
            dma((m - 1,)),
            dma((m - 1,)),
            dma((m - 1,)),
            dma((m - 1,)),
            dma((m - 1,)),
            dma((m - 1,)),
            dma((m - 1,)),
            dma((n, 2)),
            dma((m, per_owner, 2)),
        ],
        compiler_params=pltpu.CompilerParams(
            collective_id=0, has_side_effects=True, vmem_limit_bytes=60 * 1024 * 1024
        ),
        name="layer",
    )(
        queries,
        keys,
        values,
        output_gate_logits,
        gates,
        residual,
        jnp.concatenate([cell_norm_gain, mixer_norm_gain])[None, :],
        output_weight,
        up_weight,
        down_weight,
    )


def either(n, m, *args):
    depth, hidden_width = args[12].shape
    heads = args[0].shape[1] // DH
    fits = depth % 256 == 0 and n % 2 == 0 and n >= 4 and n <= 16 and m >= 2
    fits = fits and 2 * heads + 1 <= 8 and args[8].shape[1] % depth == 0
    fits = fits and args[0].shape[0] % 128 == 0 and hidden_width % 256 == 0
    if fits:
        return fused(n, m, *args)
    return local(*args)


def solution(mesh):
    in_specs = (
        P("sp", "tp"),
        P("sp", "tp"),
        P("sp", "tp"),
        P("sp", "tp"),
        P("sp", "tp"),
        P("sp", "tp"),
        P("sp", "tp"),
        P("sp"),
        P("sp", "tp"),
        P("tp"),
        P("tp", None),
        P("tp"),
        P("sp", "tp"),
        P("tp", "sp"),
    )
    out_specs = P("sp", "tp")
    body = functools.partial(either, mesh.shape["sp"], mesh.shape["tp"])
    return jax.shard_map(body, mesh=mesh, in_specs=in_specs, out_specs=out_specs, check_vma=False)
```
